128 devices in a mesh: sp: 16 (over z, y), tp: 8 (over x, core).
Axes of the slice: x: 4, y: 4, z: 4, core: 2. Of those that a mesh axis runs over, the one named last changes fastest.
Arguments:
- inputs: bfloat16 [4096, 4096], P('sp', 'tp'), may hold values from -6 to 6
- input_norm_gain: bfloat16 [4096], replicated, may hold values from 0.099609375 to 1.8984375
- pooling_input_weight: bfloat16 [4096, 2048], P('sp', 'tp'), may hold values from -0.09375 to 0.09375
- query_weight: bfloat16 [4096, 2048], P('sp', 'tp'), may hold values from -0.09375 to 0.09375
- key_weight: bfloat16 [4096, 2048], P('sp', 'tp'), may hold values from -0.09375 to 0.09375
- value_weight: bfloat16 [4096, 2048], P('sp', 'tp'), may hold values from -0.09375 to 0.09375
- gate_weight: bfloat16 [4096, 2048], P('sp', 'tp'), may hold values from -0.09375 to 0.09375
- decay_weight: bfloat16 [4096, 16], replicated, may hold values from -0.25 to 0.25
- strength_weight: bfloat16 [4096, 16], replicated, may hold values from -0.09375 to 0.09375
- pooling_group_map: bfloat16 [16, 128, 128], P('tp'), may hold values from -0.5 to 0.5
- pooling_scale: float32 [2048], P('tp'), may hold values from 0.1 to 1.9
- head_log_decay: float32 [16], P('tp')
- decay_logit_bias: float32 [16], P('tp'), may hold values from -1 to 1
- write_logit_bias: float32 [16], P('tp')
- decay_position_factor: float32 [4096, 16], P('sp', 'tp'), may hold values from 0.28 to 3.25
- decay_position_offset: float32 [4096, 16], P('sp', 'tp'), may hold values from -0.7 to 0
- head_norm_gain: float32 [128], replicated, may hold values from 0.1 to 1.9
- pooling_output_weight: bfloat16 [2048, 4096], P('tp', 'sp'), may hold values from -0.125 to 0.125
- delta_output_weight: bfloat16 [2048, 4096], P('tp', 'sp'), may hold values from -0.125 to 0.125
Outputs:
- mixed_out: bfloat16 [4096, 4096], P('sp', 'tp')
The draws below stay inside these ranges and needn't reach their ends.
All inputs are finite; a program needn't handle non-finite values.
Results may differ from the reference program's by a relative error of at most 0.02.
Values may be sent and summed in bfloat16 or wider, within the bound.
A program may use at most 128 MiB of HBM per device.

```python
import jax
import jax.numpy as jnp
from jax import lax

D = 4096
HD = 128
GH = 16
PG = 16
PC = 128
BLK = 64
TOK_DEV = 256
TOKENS = 4096
PW = 2048
GW = 2048
N_TP = 8


def speed_flags(key):
    share = 0.5
    return jax.random.bernoulli(jax.random.fold_in(key, 11), share, (GH,))


def draw_head_log_decay(key, part):
    quick_heads = speed_flags(key)
    mixing = jax.random.uniform(jax.random.fold_in(key, 12), (GH,), jnp.float32)
    quick_rate = jnp.exp(jnp.log(1.0 / 80.0) + mixing * (jnp.log(1.0 / 25.0) - jnp.log(1.0 / 80.0)))
    slow_rate = jnp.exp(jnp.log(0.03) + mixing * (jnp.log(0.15) - jnp.log(0.03))) / TOKENS
    return jnp.log(jnp.where(quick_heads, quick_rate, slow_rate)).astype(jnp.float32)


def draw_write_logit_bias(key, part):
    quick_heads = speed_flags(key)
    jitter = jax.random.uniform(jax.random.fold_in(key, 13), (GH,), jnp.float32, -0.5, 0.5)
    return jnp.where(quick_heads, jitter, jnp.log(0.3 * HD / TOKENS) + jitter).astype(jnp.float32)


def draw_decay_position_factor(key, part):
    device_count = TOKENS // TOK_DEV
    block_level = jnp.exp(jax.random.uniform(jax.random.fold_in(key, 14), (device_count, GH), jnp.float32, jnp.log(0.4), jnp.log(2.5)))
    jitter = jax.random.uniform(jax.random.fold_in(key, 15), (TOKENS, GH), jnp.float32, 0.7, 1.3)
    return (jnp.repeat(block_level, TOK_DEV, axis=0) * jitter).astype(jnp.float32)


def draw_decay_position_offset(key, part):
    places = jax.random.randint(jax.random.fold_in(key, 16), (2, GH), 0, TOKENS)
    losses = jnp.log(jax.random.uniform(jax.random.fold_in(key, 17), (2, GH), jnp.float32, 0.5, 0.8))
    hit_table = jnp.arange(TOKENS)[:, None, None] == places[None]
    return jnp.sum(jnp.where(hit_table, losses[None], 0.0), axis=1).astype(jnp.float32)


def levels(stream_key, dims, split, least, high):
    level = 1.0
    for axis_at, shards_of in split:
        draws = jax.random.uniform(jax.random.fold_in(jax.random.fold_in(stream_key, 6), axis_at), (shards_of,), jnp.float32, least / len(split), high / len(split))
        level = level * jnp.repeat(jnp.exp(draws), dims[axis_at] // shards_of).reshape((-1,) + (1,) * (len(dims) - 1 - axis_at))
    return level


def centred(rng, dims, deviation, most, shards=(), kind=jnp.bfloat16):
    result = deviation * jax.random.normal(rng, dims, jnp.float32)
    if shards:
        result = result * levels(rng, dims, shards, -0.22, 0.18)
    return jnp.clip(result, -most, most).astype(kind)


def setup_inputs(seed: int = 0) -> dict:
    splits = jax.random.split(jax.random.key(seed), 20)
    return {
        "inputs": centred(splits[0], (TOKENS, D), 1.0, 6.0, ((0, 16), (1, 8))),
        "input_norm_gain": jnp.clip(1.0 + 0.18 * jax.random.normal(splits[1], (D,), jnp.float32), 0.099609375, 1.8984375).astype(jnp.bfloat16),
        "pooling_input_weight": centred(splits[2], (D, PW), D ** -0.5, 0.09375, ((0, 16), (1, 8))),
        "query_weight": centred(splits[3], (D, GW), D ** -0.5, 0.09375, ((0, 16), (1, 8))),
        "key_weight": centred(splits[4], (D, GW), D ** -0.5, 0.09375, ((0, 16), (1, 8))),
        "value_weight": centred(splits[5], (D, GW), D ** -0.5, 0.09375, ((0, 16), (1, 8))),
        "gate_weight": centred(splits[6], (D, GW), D ** -0.5, 0.09375, ((0, 16), (1, 8))),
        "decay_weight": centred(splits[7], (D, GH), (D // 9) ** -0.5, 0.25),
        "strength_weight": centred(splits[8], (D, GH), D ** -0.5, 0.09375),
        "pooling_group_map": centred(splits[9], (PG, PC, PC), PC ** -0.5, 0.5, ((0, 8),)),
        "pooling_scale": jnp.clip(1.0 + 0.18 * jax.random.normal(splits[10], (PW,), jnp.float32), 0.1, 1.9),
        "head_log_decay": draw_head_log_decay(jax.random.fold_in(splits[19], 71), 0),
        "decay_logit_bias": jnp.clip(jax.random.uniform(splits[12], (GH,), jnp.float32, -1.0, 1.0) * levels(splits[12], (GH,), ((0, 8),), -0.4, 0.0), -1.0, 1.0),
        "write_logit_bias": draw_write_logit_bias(jax.random.fold_in(splits[19], 71), 0),
        "decay_position_factor": draw_decay_position_factor(jax.random.fold_in(splits[19], 71), 0),
        "decay_position_offset": draw_decay_position_offset(jax.random.fold_in(splits[19], 71), 0),
        "head_norm_gain": jnp.clip(1.0 + 0.18 * jax.random.normal(splits[16], (HD,), jnp.float32), 0.1, 1.9),
        "pooling_output_weight": centred(splits[17], (PW, D), PW ** -0.5, 0.125, ((0, 8), (1, 16))),
        "delta_output_weight": centred(splits[18], (GW, D), GW ** -0.5, 0.125, ((0, 8), (1, 16))),
    }


epsilon = 1e-06
highest = lax.Precision.HIGHEST

def unit_rows(matrix):
    return matrix * lax.rsqrt(lax.optimization_barrier(jnp.sum(matrix * matrix, axis=-1, keepdims=True)) + epsilon)

def pool_windows(first_group, group_count):
    group_ids = first_group + jnp.arange(group_count, dtype=jnp.int32)
    return 2 ** (1 + group_ids % 4)

def pool_branch(padded, windows, positions, pooling_group_map, pooling_scale):
    row_count = padded.shape[0] - 16
    window_sum = jnp.zeros(padded[16:].shape, jnp.float32)
    for lag_index in range(16):
        window_part = padded[16 - lag_index:16 - lag_index + row_count]
        window_sum = window_sum + window_part * (lag_index < windows).astype(jnp.float32)[None, :, None]
    counts = jnp.minimum(positions[:, None] + 1, windows[None, :]).astype(jnp.float32)
    mixed = window_sum / counts[..., None] - padded[16:]
    projected = jnp.einsum('tgc,gcd->tgd', mixed, pooling_group_map.astype(jnp.float32), precision=highest)
    return (projected.reshape(row_count, -1) * pooling_scale).astype(jnp.bfloat16)

def delta_rule_inputs(query_row_block, key_matrix_rows, value_row_block, decay_logits, write_logits, head_log_decay, decay_logit_bias, write_logit_bias, decay_position_factor, decay_position_offset):
    row_count = query_row_block.shape[0]
    head_count = head_log_decay.shape[0]

    def heads_of(matrix):
        return jax.nn.silu(matrix.astype(jnp.float32)).reshape(row_count, head_count, HD)
    query_matrix = unit_rows(heads_of(query_row_block)) * HD ** (-0.5)
    incoming_keys = unit_rows(heads_of(key_matrix_rows))
    value_matrix = heads_of(value_row_block)
    write_strength_rows = jax.nn.sigmoid(write_logits + write_logit_bias)
    decay_log_rows = -jnp.exp(head_log_decay) * jax.nn.softplus(decay_logits + decay_logit_bias) * decay_position_factor + decay_position_offset
    return (query_matrix, incoming_keys, value_matrix, write_strength_rows, decay_log_rows)

def block_terms(query_matrix, incoming_keys, value_matrix, write_strength_rows, decay_log_rows):
    length, head_count, head_depth = query_matrix.shape
    blocks = length // BLK

    def regroup(member):
        return member.reshape(blocks, BLK, head_count, -1).transpose(2, 0, 1, 3)
    query_matrix, incoming_keys, value_matrix = (regroup(query_matrix), regroup(incoming_keys), regroup(value_matrix))
    write_strength_rows = write_strength_rows.reshape(blocks, BLK, head_count).transpose(2, 0, 1)
    running = jnp.cumsum(decay_log_rows.reshape(blocks, BLK, head_count).transpose(2, 0, 1), axis=-1)
    positions = jnp.arange(BLK)
    causal = positions[:, None] >= positions[None, :]
    strict = positions[:, None] > positions[None, :]
    spread = running[..., :, None] - running[..., None, :]
    decay_table = jnp.where(causal, jnp.exp(jnp.where(causal, spread, 0.0)), 0.0)
    weighted = incoming_keys * write_strength_rows[..., None]
    lower_part = jnp.where(strict, jnp.einsum('hnid,hnjd->hnij', weighted, incoming_keys, precision=highest) * decay_table, 0.0)
    system = lower_part + jnp.eye(BLK, dtype=jnp.float32)
    corrected = jax.scipy.linalg.solve_triangular(system, value_matrix * write_strength_rows[..., None], lower=True)
    erased = jax.scipy.linalg.solve_triangular(system, weighted * jnp.exp(running)[..., None], lower=True)
    scores = jnp.einsum('hnid,hnjd->hnij', query_matrix, incoming_keys, precision=highest) * decay_table
    query_decayed = query_matrix * jnp.exp(running)[..., None]
    block_total = running[..., -1]
    key_decayed = incoming_keys * jnp.exp(block_total[..., None] - running)[..., None]
    return (corrected, erased, query_decayed, key_decayed, scores, block_total)

def run_blocks(state_start, terms):

    def advance(state_now, pieces):
        corrected, erased, query_decayed, key_decayed, scores, block_total = pieces
        fresh_values = corrected - jnp.einsum('hcd,hde->hce', erased, state_now, precision=highest)
        output = jnp.einsum('hcd,hde->hce', query_decayed, state_now, precision=highest)
        output = output + jnp.einsum('hij,hje->hie', scores, fresh_values, precision=highest)
        state_now = state_now * jnp.exp(block_total)[:, None, None]
        state_now = state_now + jnp.einsum('hcd,hce->hde', key_decayed, fresh_values, precision=highest)
        return (state_now, output)
    stacked = tuple((jnp.moveaxis(member, 1, 0) for member in terms))
    final_state, outputs = lax.scan(advance, state_start, stacked)
    blocks, head_count, block_rows, head_depth = outputs.shape
    return (final_state, outputs.transpose(0, 2, 1, 3).reshape(blocks * block_rows, head_count, head_depth))

def delta_finish(outputs, gate_rows, head_norm_gain):
    row_count, head_count, head_depth = outputs.shape
    scaled = outputs * lax.rsqrt(lax.optimization_barrier(jnp.mean(outputs * outputs, axis=-1, keepdims=True)) + epsilon) * head_norm_gain
    gated = scaled * jax.nn.silu(gate_rows.astype(jnp.float32).reshape(row_count, head_count, head_depth))
    return gated.reshape(row_count, head_count * head_depth).astype(jnp.bfloat16)

def reference(inputs, input_norm_gain, pooling_input_weight, query_weight, key_weight, value_weight, gate_weight, decay_weight, strength_weight, pooling_group_map, pooling_scale, head_log_decay, decay_logit_bias, write_logit_bias, decay_position_factor, decay_position_offset, head_norm_gain, pooling_output_weight, delta_output_weight):
    floats = inputs.astype(jnp.float32)
    normed = (floats * lax.rsqrt(lax.optimization_barrier(jnp.mean(floats * floats, axis=-1, keepdims=True)) + epsilon) * input_norm_gain.astype(jnp.float32)).astype(jnp.bfloat16)
    pool_rows = jnp.dot(normed.astype(jnp.float32), pooling_input_weight.astype(jnp.float32), preferred_element_type=jnp.float32).astype(jnp.bfloat16)
    query_row_block = jnp.dot(normed.astype(jnp.float32), query_weight.astype(jnp.float32), preferred_element_type=jnp.float32).astype(jnp.bfloat16)
    key_matrix_rows = jnp.dot(normed.astype(jnp.float32), key_weight.astype(jnp.float32), preferred_element_type=jnp.float32).astype(jnp.bfloat16)
    value_row_block = jnp.dot(normed.astype(jnp.float32), value_weight.astype(jnp.float32), preferred_element_type=jnp.float32).astype(jnp.bfloat16)
    gate_rows = jnp.dot(normed.astype(jnp.float32), gate_weight.astype(jnp.float32), preferred_element_type=jnp.float32).astype(jnp.bfloat16)
    decay_logits = jnp.dot(normed.astype(jnp.float32), decay_weight.astype(jnp.float32), preferred_element_type=jnp.float32)
    write_logits = jnp.dot(normed.astype(jnp.float32), strength_weight.astype(jnp.float32), preferred_element_type=jnp.float32)
    total_rows = inputs.shape[0]
    padded = jnp.pad(pool_rows.astype(jnp.float32), ((16, 0), (0, 0))).reshape(total_rows + 16, PG, PC)
    pool_out = pool_branch(padded, pool_windows(0, PG), jnp.arange(total_rows, dtype=jnp.int32), pooling_group_map, pooling_scale)
    query_matrix, incoming_keys, value_matrix, write_strength_rows, decay_log_rows = delta_rule_inputs(query_row_block, key_matrix_rows, value_row_block, decay_logits, write_logits, head_log_decay, decay_logit_bias, write_logit_bias, decay_position_factor, decay_position_offset)
    terms = block_terms(query_matrix, incoming_keys, value_matrix, write_strength_rows, decay_log_rows)
    final_state, outputs = run_blocks(jnp.zeros((GH, HD, HD), jnp.float32), terms)
    delta_out = delta_finish(outputs, gate_rows, head_norm_gain)
    pool_group = PW // N_TP
    delta_group = GW // N_TP
    mixed = jnp.zeros((total_rows, D), jnp.float32)
    for group_index in range(N_TP):
        pool_part = jnp.dot(pool_out[:, group_index * pool_group:(group_index + 1) * pool_group].astype(jnp.float32), pooling_output_weight[group_index * pool_group:(group_index + 1) * pool_group].astype(jnp.float32), preferred_element_type=jnp.float32)
        delta_part = jnp.dot(delta_out[:, group_index * delta_group:(group_index + 1) * delta_group].astype(jnp.float32), delta_output_weight[group_index * delta_group:(group_index + 1) * delta_group].astype(jnp.float32), preferred_element_type=jnp.float32)
        rounded = lax.optimization_barrier((pool_part + delta_part).astype(jnp.bfloat16))
        mixed = mixed + rounded.astype(jnp.float32)
    return mixed.astype(jnp.bfloat16)
```

```python
import functools

import jax
import jax.numpy as jnp
from jax import lax
from jax.experimental import pallas as pl
from jax.experimental.pallas import tpu as pltpu
from jax.sharding import PartitionSpec as P

MESH = pl.DeviceIdType.MESH
F32 = jnp.float32
BF16 = jnp.bfloat16
HD = 128
EPS = 1e-06
HIGHEST = lax.Precision.HIGHEST


def dot(a, b, dims=((1,), (0,)), precision=None):
    return lax.dot_general(
        a, b, (dims, ((), ())), precision=precision, preferred_element_type=F32
    )


def iota(shape, dim):
    return lax.broadcasted_iota(jnp.int32, shape, dim)


def silu(a):
    return a * jax.nn.sigmoid(a)


def unit(a):
    return a * lax.rsqrt(jnp.sum(a * a, axis=-1, keepdims=True) + EPS)


def kernel(
    x_in, wp_in, wq_in, wk_in, wv_in, wg_in, op_in, od_in, pk_in, pm_in,
    pk_v, dw_v, sw_v,
    out_ref,
    xbuf, wbuf, wo, packb, pmb, xg, acc, ssq,
    stc, stz_src, stz, pad, pool_src, delta_src, prev_src, ap, ad,
    rs2, rsp, rsm, rl, rin, o0, pmx, kw0_s, b0_s, keep_s, low_s, inv_s, up_s, down_s, state_s,
    x_rs, w_rs, wo_rs, pk_rs, pm_rs, st_rs, stz_rs, prev_rs, ap_rs, ad_rs, rs_rs,
    x_ss, xf_ss, w_ss, wf_ss, wo_ss, wof_ss, pk_ss, pm_ss, st_ss, stz_ss, prev_ss,
    ap_ss, ad_ss, apf_ss, adf_ss, rs_ss,
):
    sp, tp = lax.axis_index("sp"), lax.axis_index("tp")
    z, y = lax.div(sp, 4), lax.rem(sp, 4)
    x, c = lax.div(tp, 2), lax.rem(tp, 2)
    kh = lax.div(y, 2)
    yodd = lax.rem(y, 2)
    home = c == kh
    away = jnp.logical_not(home)

    def mod4(a):
        return lax.rem(a + 8, 4)

    def dev(zz, yy, xx, cc):
        return (4 * zz + yy, 2 * xx + cc)

    zp, zm, z2 = mod4(z + 1), mod4(z - 1), mod4(z + 2)
    yp, ym = mod4(y + 1), mod4(y - 1)
    xp, xm, x2 = mod4(x + 1), mod4(x - 1), mod4(x + 2)
    me_z, me_y, me_x = z, y, x
    partner = dev(z, y, x, 1 - c)

    ends = []

    def remote(src, dst, ssem, rsem, to, cond=None):
        def make():
            return pltpu.make_async_remote_copy(
                src_ref=src, dst_ref=dst, send_sem=ssem, recv_sem=rsem,
                device_id=to, device_id_type=MESH,
            )

        if cond is None:
            make().start()
            ends.append(lambda: make().wait_send())
        else:
            @pl.when(cond)
            def _():
                make().start()

            def end():
                @pl.when(cond)
                def _():
                    make().wait_send()

            ends.append(end)

    def arrived(ref, sem):
        pltpu.make_async_copy(ref, ref, sem).wait()

    barrier = pltpu.get_barrier_semaphore()
    peers = [partner]
    for d in (1, 2, 3):
        for cc in (0, 1):
            peers.append(dev(mod4(z + d), y, x, cc))
            peers.append(dev(z, mod4(y + d), x, cc))
            peers.append(dev(z, y, mod4(x + d), cc))
    for to in peers:
        pl.semaphore_signal(barrier, inc=1, device_id=to, device_id_type=MESH)
    pl.semaphore_wait(barrier, len(peers))

    def xslot(yy, xx, cc):
        return xbuf.at[2 * xx + cc, pl.ds(256 * lax.rem(yy, 2), 256), :]

    def xsem(yy, xx, cc):
        return x_rs.at[8 * lax.rem(yy, 2) + 2 * xx + cc]

    def wslot(zz, yy, r):
        return wbuf.at[2 * (4 * zz + yy) + r, :, pl.ds(0, 640)]

    def wsem(zz, yy, r):
        return w_rs.at[2 * (4 * zz + yy) + r]

    def woslot(zz, yy, cc):
        return wo.at[zz, 2 * lax.rem(yy, 2) + cc]

    def wosem(zz, yy, cc):
        return wo_rs.at[4 * zz + 2 * lax.rem(yy, 2) + cc]

    own = xslot(y, x, c)
    own_sem = xsem(y, x, c)
    remote(x_in, own, x_ss.at[0], own_sem, dev(z, y, xp, kh))
    remote(x_in, own, x_ss.at[1], own_sem, dev(z, y, xm, kh))
    remote(x_in, own, x_ss.at[2], own_sem, dev(z, yp, x, kh))
    remote(x_in, own, x_ss.at[3], own_sem, dev(z, ym, x, kh))
    remote(x_in, own, x_ss.at[4], own_sem, partner, away)

    @pl.when(home)
    def _():
        pltpu.make_async_copy(x_in, own, own_sem).start()

    wo_own = woslot(z, y, c)
    for half, ref in enumerate((op_in, od_in)):
        part = wo_own.at[pl.ds(256 * half, 256), :]
        for i, zz in enumerate((zp, zm)):
            remote(ref, part, wo_ss.at[2 * half + i], wosem(z, y, c), dev(zz, y, x, kh))
        remote(ref, part, wo_ss.at[4 + half], wosem(z, y, c), partner, away)

        @pl.when(home)
        def _(ref=ref, part=part):
            pltpu.make_async_copy(ref, part, wosem(z, y, c)).start()

    for j in (0, 1):
        head_y = 2 * c + j
        for r in (0, 1):
            self_here = jnp.logical_and(head_y == y, c == r)
            for n, ref in enumerate((wp_in, wq_in, wk_in, wv_in, wg_in)):
                src = ref.at[pl.ds(128 * r, 128), pl.ds(128 * j, 128)]
                dst = wbuf.at[2 * sp + r, :, pl.ds(128 * n, 128)]
                remote(
                    src, dst, w_ss.at[5 * (2 * j + r) + n], wsem(z, y, r),
                    dev(z, head_y, x, r), jnp.logical_not(self_here),
                )

                @pl.when(self_here)
                def _(src=src, dst=dst, r=r):
                    pltpu.make_async_copy(src, dst, wsem(z, y, r)).start()

    for j in (0, 1):
        head_y = 2 * c + j
        self_here = jnp.logical_and(head_y == y, home)
        src = pk_in.at[pl.ds(8, 16), :]
        dst = packb.at[yodd]
        remote(
            src, dst, pk_ss.at[j], pk_rs.at[yodd], dev(z, head_y, x, kh),
            jnp.logical_not(self_here),
        )

        @pl.when(self_here)
        def _(src=src, dst=dst):
            pltpu.make_async_copy(src, dst, pk_rs.at[yodd]).start()

    remote(pm_in.at[yodd], pmb, pm_ss.at[0], pm_rs.at[0], partner, home)

    @pl.when(home)
    def _():
        pltpu.make_async_copy(pm_in.at[yodd], pmb, pm_rs.at[0]).start()

    head = 4 * x + y
    row16, col16 = iota((16, 128), 0), iota((16, 128), 1)
    pick_d = jnp.logical_and(row16 == head, col16 == 0).astype(BF16)
    pick_s = jnp.logical_and(row16 == head, col16 == 1).astype(BF16)

    def fill(i, carry):
        rows = pl.ds(pl.multiple_of(128 * i, 128), 128)
        both = dot(dw_v[rows, :], pick_d) + dot(sw_v[rows, :], pick_s)
        wbuf[i, :, 640:768] = both.astype(BF16)
        return carry

    lax.fori_loop(0, 32, fill, 0)

    def w_first(d, n):
        yy = mod4(me_y + d)
        slot = wslot(me_z, yy, c)
        arrived(slot, wsem(me_z, yy, c))
        remote(slot, slot, wf_ss.at[n], wsem(me_z, yy, c), dev(zp, y, x, c))
        remote(slot, slot, wf_ss.at[n + 1], wsem(me_z, yy, c), dev(zm, y, x, c))
        remote(slot, slot, wf_ss.at[n + 2], wsem(me_z, yy, c), partner)

    def w_later(zz, d, n, to_z=None):
        yy = mod4(me_y + d)
        slot = wslot(zz, yy, c)
        arrived(slot, wsem(zz, yy, c))
        if to_z is not None:
            remote(slot, slot, wf_ss.at[n + 1], wsem(zz, yy, c), dev(to_z, y, x, c))
        remote(slot, slot, wf_ss.at[n], wsem(zz, yy, c), partner)

    yn = 2 * c + 1 - yodd
    yo = 2 * c + yodd
    from_below = mod4(yn + 1) == y
    relay_c = jnp.where(from_below, 0, 1)
    y_next = jnp.where(from_below, yp, ym)

    w_first(0, 0)
    for cc in (0, 1):
        slot = xslot(yn, x, cc)
        arrived(slot, xsem(yn, x, cc))
        remote(slot, slot, xf_ss.at[2 * cc], xsem(yn, x, cc), dev(z, y, xp, c))
        remote(slot, slot, xf_ss.at[2 * cc + 1], xsem(yn, x, cc), dev(z, y, xm, c))
    slot = xslot(yn, x, relay_c)
    remote(slot, slot, xf_ss.at[4], xsem(yn, x, relay_c), dev(z, y_next, x, c))
    w_first(1, 3)
    w_first(3, 6)
    for cc in (0, 1):
        slot = xslot(yo, x, cc)
        arrived(slot, xsem(yo, x, cc))
        remote(slot, slot, xf_ss.at[5 + 2 * cc], xsem(yo, x, cc), dev(z, y, xp, c), away)
        remote(slot, slot, xf_ss.at[6 + 2 * cc], xsem(yo, x, cc), dev(z, y, xm, c), away)
    w_first(2, 9)

    yf = jnp.where(home, yo, yn)
    yl = jnp.where(home, yn, yo)
    n = 9
    for yy in (yf, yl):
        for xx, cc, to_x in ((xm, 0, xp), (xp, 1, xm)):
            slot = xslot(yy, xx, cc)
            arrived(slot, xsem(yy, xx, cc))
            remote(slot, slot, xf_ss.at[n], xsem(yy, xx, cc), dev(z, y, to_x, c))
            n += 1

    def wo_home(zz, cc, n, to_z=None):
        @pl.when(home)
        def _():
            slot = woslot(zz, me_y, cc)
            arrived(slot, wosem(zz, me_y, cc))

        slot = woslot(zz, me_y, cc)
        sem = wosem(zz, me_y, cc)
        if to_z is not None:
            remote(slot, slot, wof_ss.at[n], sem, dev(to_z, y, x, c), home)
        remote(slot, slot, wof_ss.at[n + 1], sem, dev(z, yp, x, c), home)
        remote(slot, slot, wof_ss.at[n + 2], sem, dev(z, ym, x, c), home)

    wo_home(z, 0, 0)
    wo_home(z, 1, 3)
    wo_home(zm, 0, 6, zp)
    wo_home(zp, 1, 9, zm)

    n = 12
    for d in (0, 1, 3, 2):
        w_later(zm, d, n, zp if d in (0, 2) else None)
        w_later(zp, d, n + 2, zm if d in (1, 3) else None)
        n += 4

    wo_home(zm, 1, 12)
    wo_home(zp, 0, 15)
    wo_home(z2, 0, 18)
    wo_home(z2, 1, 21)

    for d in (0, 1, 3, 2):
        w_later(z2, d, n)
        n += 1

    for yy in (yn, yo):
        for xx, cc in ((xm, 1), (xp, 0), (x2, 0), (x2, 1)):
            arrived(xslot(yy, xx, cc), xsem(yy, xx, cc))
    for zz in (z, zp, zm, z2):
        for d in (0, 1, 2, 3):
            yy = mod4(y + d)
            arrived(wslot(zz, yy, 1 - c), wsem(zz, yy, 1 - c))

    ssq[...] = jnp.zeros_like(ssq)
    acc[...] = jnp.zeros_like(acc)

    def project(i, carry):
        gain = pk_v[pl.ds(i, 1), :]
        for b in range(4):
            rows = slice(128 * b, 128 * b + 128)
            v = xbuf[i, rows, :].astype(F32)
            sq = v * v
            ssq[rows, :] += (
                (sq[:, 0:128] + sq[:, 128:256]) + (sq[:, 256:384] + sq[:, 384:512])
            )
            xg[rows, :] = (v * gain).astype(BF16)
        acc[...] += dot(xg[...], wbuf[pl.ds(4 * i, 4)].reshape(512, 768))
        return carry

    lax.fori_loop(0, 8, project, 0)

    def wo_away_pump(zs, n):
        for zz in zs:
            for cc in (0, 1):
                arrived(woslot(zz, yn, cc), wosem(zz, yn, cc))
            slot = woslot(zz, yn, relay_c)
            remote(slot, slot, wof_ss.at[n], wosem(zz, yn, relay_c), dev(z, y_next, x, c))
            n += 1

    wo_away_pump((z, zm), 24)

    for b in (0, 1):
        arrived(packb.at[b], pk_rs.at[b])
    arrived(pmb, pm_rs.at[0])

    ii, jj = iota((256, 256), 0), iota((256, 256), 1)
    diff = jnp.bitwise_xor(ii, jj)
    lower = ii > jj
    causal = ii >= jj
    upto = (ii <= jj).astype(F32)
    eye = (ii == jj).astype(F32)

    def row_scale(b):
        total = jnp.sum(ssq[256 * b : 256 * b + 256, :], axis=-1, keepdims=True)
        return lax.rsqrt(total * (1.0 / 4096.0) + EPS)

    scale = [row_scale(0), row_scale(1)]

    for b in (0, 1):
        pad[16 + 256 * b : 272 + 256 * b, :] = acc[256 * b : 256 * b + 256, 0:128] * scale[b]
    prev_src[...] = pad[512:528, :].astype(BF16)
    prev_to = dev(jnp.where(c == 0, z, zp), y, x, 1 - c)
    last = jnp.logical_and(z == 3, c == 1)
    first = jnp.logical_and(z == 0, c == 0)
    prev_dst = ap.at[pl.ds(256, 16), pl.ds(0, 128)]
    remote(prev_src, prev_dst, prev_ss.at[0], prev_rs.at[0], prev_to, jnp.logical_not(last))

    heads = []
    for b in (0, 1):
        rows = slice(256 * b, 256 * b + 256)
        s = scale[b]
        q = unit(silu(acc[rows, 128:256] * s)) * HD ** (-0.5)
        k = unit(silu(acc[rows, 256:384] * s))
        v = silu(acc[rows, 384:512] * s)
        rate = acc[rows, 640:768] * s
        table = packb[b]
        pick = lambda r: jnp.where(yodd == 0, table[r : r + 1, 0:256], table[r + 1 : r + 2, 0:256])
        factor, offset, hld, dlb, wlb = (pick(r) for r in (0, 2, 4, 6, 8))
        pre = rate.T[0:1, :] + dlb
        soft = jnp.maximum(pre, 0.0) + jnp.log1p(jnp.exp(-jnp.abs(pre)))
        log_decay = -jnp.exp(hld) * soft * factor + offset
        run_row = dot(jnp.broadcast_to(log_decay, (8, 256)), upto, precision=HIGHEST)[0:1, :]
        run = jnp.broadcast_to(run_row, (128, 256)).T
        beta = jax.nn.sigmoid(rate[:, 1:2] + wlb[:, 0:1])
        spread = jnp.concatenate([run, run], axis=1) - run_row
        decay = jnp.where(causal, jnp.exp(jnp.where(causal, spread, 0.0)), 0.0)
        k16, q16 = k.astype(BF16), q.astype(BF16)
        low = jnp.where(lower, dot(k16, k16, ((1,), (1,))) * (decay * beta), 0.0)
        scores = (dot(q16, k16, ((1,), (1,))) * decay).astype(BF16)
        inverse = eye - jnp.where(diff == 1, low, 0.0)
        grown = jnp.exp(run)
        kb = k * beta
        low_s[b] = low
        inv_s[b] = inverse
        heads.append(dict(q=q, k=k, v=v, scores=scores, run=run, grown=grown, kb=kb, beta=beta))

    for level in range(1, 8):
        mask = jnp.right_shift(diff, level) == 1
        mids = []
        for b in (0, 1):
            off = jnp.where(mask, low_s[b], 0.0).astype(BF16)
            mids.append(dot(off, inv_s[b].astype(BF16)).astype(BF16))
        for b, mid in enumerate(mids):
            inv_s[b] = inv_s[b] - dot(inv_s[b].astype(BF16), mid)

    maps = []
    for b, h in enumerate(heads):
        rows = slice(256 * b, 256 * b + 256)
        rhs = jnp.concatenate([h["v"] * h["beta"], h["kb"] * h["grown"]], axis=1)
        uw = rhs + dot((inv_s[b] - eye).astype(BF16), rhs.astype(BF16))
        uw16 = uw.astype(BF16)
        both = dot(h["scores"], uw16)
        o0[rows, :] = both[:, 0:128]
        pmx[rows, :] = (h["q"] * h["grown"] - both[:, 128:256]).astype(BF16)
        last_run = h["run"][255:256, :]
        kd = (h["k"] * jnp.exp(last_run - h["run"])).astype(BF16)
        ku = dot(kd, uw16, ((0,), (0,)))
        keep = jnp.exp(last_run)
        maps.append((keep, ku[:, 128:256].astype(BF16), ku[:, 0:128]))

    eye128 = (iota((128, 128), 0) == iota((128, 128), 1)).astype(F32)
    keep0, kw0, b0 = maps[0]
    keep1, kw1, b1 = maps[1]
    m0 = eye128 * keep0 - kw0.astype(F32)
    kw0_s[...] = kw0
    b0_s[...] = b0
    keep_s[0:1, :] = keep0
    first_map = jnp.concatenate([m0, b0], axis=1)
    keep1w = jnp.concatenate([keep1, keep1], axis=1)
    core_map = keep1w * first_map - dot(kw1, first_map.astype(BF16))
    core_map = core_map + jnp.concatenate([jnp.zeros_like(b1), b1], axis=1)
    stc[c] = core_map.astype(BF16)
    remote(stc.at[c], stc.at[c], st_ss.at[0], st_rs.at[c], partner)
    arrived(stc.at[1 - c], st_rs.at[1 - c])
    one = stc[1]
    chip_map = dot(one[:, 0:128], stc[0])
    chip_map = chip_map + jnp.concatenate([jnp.zeros_like(b1), one[:, 128:256].astype(F32)], axis=1)
    stz_src[...] = chip_map.astype(BF16)
    for d in (1, 2, 3):
        remote(
            stz_src, stz.at[z], stz_ss.at[d - 1], stz_rs.at[z],
            dev(mod4(z + d), y, x, c), z + d <= 3,
        )

    wo_away_pump((zp, z2), 26)

    @pl.when(first)
    def _():
        pad[0:16, :] = jnp.zeros((16, 128), F32)

    @pl.when(jnp.logical_not(first))
    def _():
        arrived(prev_dst, prev_rs.at[0])
        pad[0:16, :] = ap[256:272, 0:128].astype(F32)

    window = jnp.left_shift(2, y)
    base = 512 * (2 * z + c)
    for b in (0, 1):
        at = 256 * b
        sums = pad[16 + at : 272 + at, :]
        here = sums
        for lag in range(1, 16):
            part = pad[16 + at - lag : 272 + at - lag, :]
            sums = sums + part * jnp.where(lag < window, 1.0, 0.0)
        counts = jnp.minimum(base + at + iota((256, 128), 0) + 1, window).astype(F32)
        pooled = (sums / counts - here).astype(BF16)
        row = packb[b]
        pscale = jnp.where(yodd == 0, row[10:11, 0:128], row[10:11, 128:256])
        pool_src[at : at + 256, :] = (dot(pooled, pmb[...]) * pscale).astype(BF16)

    def spread_out(src, dst, rsem, ssem):
        cols = pl.ds(128 * y, 128)

        @pl.when(home)
        def _():
            dst[0:256, cols] = src[pl.ds(256 * yodd, 256), :]

        for j in (0, 1):
            to_y = 2 * c + j
            here = to_y == y
            rows = pl.ds(256 * j, 256)
            remote(
                src.at[rows, :], dst.at[pl.ds(0, 256), cols], ssem.at[3 * j],
                rsem.at[y], partner, here,
            )
            for r in (0, 1):
                remote(
                    src.at[pl.ds(256 * j + 128 * r, 128), :],
                    dst.at[pl.ds(128 * r, 128), cols],
                    ssem.at[3 * j + 1 + r], rsem.at[y], dev(z, to_y, x, r),
                    jnp.logical_not(here),
                )

    def gather_in(dst, rsem, fsem):
        for i, d in enumerate((1, 3, 2)):
            yy = mod4(me_y + d)
            part = dst.at[pl.ds(128 * c, 128), pl.ds(128 * yy, 128)]
            arrived(part, rsem.at[yy])
            remote(part, part, fsem.at[i], rsem.at[4 + yy], partner)
        for d in (1, 3, 2):
            yy = mod4(me_y + d)
            part = dst.at[pl.ds(128 * (1 - c), 128), pl.ds(128 * yy, 128)]
            arrived(part, rsem.at[4 + yy])

        @pl.when(away)
        def _():
            arrived(dst.at[pl.ds(0, 256), pl.ds(128 * me_y, 128)], rsem.at[me_y])

    spread_out(pool_src, ap, ap_rs, ap_ss)

    state_s[...] = jnp.zeros((128, 128), F32)

    def absorb(part):
        moved = dot(part[:, 0:128], state_s[...].astype(BF16))
        state_s[...] = moved + part[:, 128:256].astype(F32)

    for i in (0, 1, 2):
        @pl.when(i < z)
        def _(i=i):
            arrived(stz.at[i], stz_rs.at[i])
            absorb(stz[i])

    @pl.when(c == 1)
    def _():
        absorb(stc[0])

    hng = pk_v[24:25, 0:128]
    for b in (0, 1):
        rows = slice(256 * b, 256 * b + 256)
        s16 = state_s[...].astype(BF16)
        o = o0[rows, :] + dot(pmx[rows, :], s16)
        gate = silu(acc[rows, 512:640] * row_scale(b))
        norm = lax.rsqrt(jnp.mean(o * o, axis=-1, keepdims=True) + EPS)
        delta_src[rows, :] = (o * norm * hng * gate).astype(BF16)
        if b == 0:
            state_s[...] = keep_s[0:1, :] * state_s[...] - dot(kw0_s[...], s16) + b0_s[...]

    spread_out(delta_src, ad, ad_rs, ad_ss)

    for zz in (z, zm, zp, z2):
        for cc in (0, 1):
            @pl.when(away)
            def _(zz=zz, cc=cc):
                arrived(woslot(zz, yo, cc), wosem(zz, yo, cc))

    gather_in(ap, ap_rs, apf_ss)
    gather_in(ad, ad_rs, adf_ss)

    def piece(zz):
        halves = []
        for j in (0, 1):
            part = None
            for cc in (0, 1):
                cols = slice(256 * cc, 256 * cc + 256)
                term = dot(ap[0:256, cols], wo[zz, 2 * j + cc, 0:256, :])
                term = term + dot(ad[0:256, cols], wo[zz, 2 * j + cc, 256:512, :])
                part = term if part is None else part + term
            halves.append(part)
        return jnp.concatenate(halves, axis=1)

    top, bottom = pl.ds(0, 128), pl.ds(128, 128)
    to_p, to_m = dev(z, y, xp, c), dev(z, y, xm, c)
    rs2[...] = piece(x2).astype(BF16)
    remote(rs2.at[top, :], rl.at[0], rs_ss.at[0], rs_rs.at[0], to_p)
    remote(rs2.at[bottom, :], rl.at[1], rs_ss.at[1], rs_rs.at[1], to_m)
    up_s[...] = piece(xp)
    rsp[128:256, :] = up_s[128:256, :].astype(BF16)
    remote(rsp.at[bottom, :], rin.at[0, bottom, :], rs_ss.at[2], rs_rs.at[2], to_p)
    down_s[...] = piece(xm)
    rsm[0:128, :] = down_s[0:128, :].astype(BF16)
    remote(rsm.at[top, :], rin.at[1, top, :], rs_ss.at[3], rs_rs.at[3], to_m)
    arrived(rl.at[0], rs_rs.at[0])
    rsp[0:128, :] = (up_s[0:128, :] + rl[0].astype(F32)).astype(BF16)
    remote(rsp.at[top, :], rin.at[0, top, :], rs_ss.at[4], rs_rs.at[4], to_p)
    arrived(rl.at[1], rs_rs.at[1])
    rsm[128:256, :] = (down_s[128:256, :] + rl[1].astype(F32)).astype(BF16)
    remote(rsm.at[bottom, :], rin.at[1, bottom, :], rs_ss.at[5], rs_rs.at[5], to_m)
    mine = piece(x)
    arrived(rin.at[0, bottom, :], rs_rs.at[2])
    arrived(rin.at[1, top, :], rs_rs.at[3])
    arrived(rin.at[0, top, :], rs_rs.at[4])
    arrived(rin.at[1, bottom, :], rs_rs.at[5])
    out_ref[...] = (mine + rin[0].astype(F32) + rin[1].astype(F32)).astype(BF16)

    for end in ends:
        end()


def per_device(
    inputs, input_norm_gain, pooling_input_weight, query_weight, key_weight,
    value_weight, gate_weight, decay_weight, strength_weight, pooling_group_map,
    pooling_scale, head_log_decay, decay_logit_bias, write_logit_bias,
    decay_position_factor, decay_position_offset, head_norm_gain,
    pooling_output_weight, delta_output_weight,
):
    def wide(rows):
        rows = rows.astype(F32)
        return jnp.pad(rows, ((0, 0), (0, 512 - rows.shape[1])))

    def level(a):
        return wide(jnp.broadcast_to(a[:, None], (2, 256)))

    table = jnp.concatenate(
        [
            input_norm_gain.astype(F32).reshape(8, 512),
            wide(decay_position_factor.T),
            wide(decay_position_offset.T),
            level(head_log_decay),
            level(decay_logit_bias),
            level(write_logit_bias),
            wide(pooling_scale[None]),
            jnp.zeros((5, 512), F32),
            wide(head_norm_gain[None]),
            jnp.zeros((7, 512), F32),
        ],
        axis=0,
    )
    dma = pltpu.SemaphoreType.DMA
    vmem = pltpu.VMEM
    hbm = pl.BlockSpec(memory_space=pl.ANY)
    local = pl.BlockSpec(memory_space=pltpu.VMEM)
    return pl.pallas_call(
        kernel,
        out_shape=jax.ShapeDtypeStruct((256, 512), BF16),
        in_specs=[hbm] * 10 + [local] * 3,
        out_specs=local,
        scratch_shapes=[
            vmem((8, 512, 512), BF16),
            vmem((32, 128, 768), BF16),
            vmem((4, 4, 512, 256), BF16),
            vmem((2, 16, 512), F32),
            vmem((128, 128), BF16),
            vmem((512, 512), BF16),
            vmem((512, 768), F32),
            vmem((512, 128), F32),
            vmem((2, 128, 256), BF16),
            vmem((128, 256), BF16),
            vmem((4, 128, 256), BF16),
            vmem((528, 128), F32),
            vmem((512, 128), BF16),
            vmem((512, 128), BF16),
            vmem((16, 128), BF16),
            vmem((272, 512), BF16),
            vmem((256, 512), BF16),
            vmem((256, 512), BF16),
            vmem((256, 512), BF16),
            vmem((256, 512), BF16),
            vmem((2, 128, 512), BF16),
            vmem((2, 256, 512), BF16),
            vmem((512, 128), F32),
            vmem((512, 128), BF16),
            vmem((128, 128), BF16),
            vmem((128, 128), F32),
            vmem((8, 128), F32),
            vmem((2, 256, 256), F32),
            vmem((2, 256, 256), F32),
            vmem((256, 512), F32),
            vmem((256, 512), F32),
            vmem((128, 128), F32),
            dma((16,)), dma((32,)), dma((16,)), dma((2,)), dma((1,)), dma((2,)),
            dma((4,)), dma((1,)), dma((8,)), dma((8,)), dma((6,)),
            dma((5,)), dma((13,)), dma((20,)), dma((32,)), dma((6,)), dma((28,)),
            dma((2,)), dma((1,)), dma((1,)), dma((3,)), dma((1,)),
            dma((6,)), dma((6,)), dma((3,)), dma((3,)), dma((6,)),
        ],
        compiler_params=pltpu.CompilerParams(
            collective_id=0, has_side_effects=True, vmem_limit_bytes=60 * 1024 * 1024
        ),
    )(
        inputs, pooling_input_weight, query_weight, key_weight, value_weight,
        gate_weight, pooling_output_weight, delta_output_weight, table,
        pooling_group_map, table, decay_weight, strength_weight,
    )


def solution(mesh):
    rows, heads = P("sp", "tp"), P("tp")
    in_specs = (
        rows, P(), rows, rows, rows, rows, rows, P(), P(), P("tp", None, None),
        heads, heads, heads, heads, rows, rows, P(), P("tp", "sp"), P("tp", "sp"),
    )
    return jax.shard_map(
        per_device, mesh=mesh, in_specs=in_specs, out_specs=rows, check_vma=False
    )
```

```python
import functools

import jax
import jax.numpy as jnp
from jax import lax
from jax.experimental import pallas as pl
from jax.experimental.pallas import tpu as pltpu
from jax.sharding import PartitionSpec as P

MESH = pl.DeviceIdType.MESH
F32 = jnp.float32
BF16 = jnp.bfloat16
HD = 128
EPS = 1e-06
HIGHEST = lax.Precision.HIGHEST


def dot(a, b, dims=((1,), (0,)), precision=None):
    return lax.dot_general(
        a, b, (dims, ((), ())), precision=precision, preferred_element_type=F32
    )


def iota(shape, dim):
    return lax.broadcasted_iota(jnp.int32, shape, dim)


def silu(a):
    return a * jax.nn.sigmoid(a)


def unit(a):
    return a * lax.rsqrt(jnp.sum(a * a, axis=-1, keepdims=True) + EPS)


def kernel(
    x_in, wp_in, wq_in, wk_in, wv_in, wg_in, op_in, od_in, pm_in,
    hld_in, dlb_in, wlb_in, gain_in, factor_in, offset_in, pscale_in, hng_in, dw_in, sw_in,
    out_ref,
    hld_v, dlb_v, wlb_v, gain_v, factor_v, offset_v, pscale_v, hng_v, rates_v,
    xbuf, wbuf, wo, gain_f, pk_src, packb, pmb, xg, acc, ssq,
    w_stage, stc, stz_src, stz, pad, pool_src, delta_src, prev_src, ap, ad,
    rs2, rsp, rsm, rl, rin, o0, pmx, kw0_s, b0_s, keep_s, low_s, inv_s, up_s, down_s, state_s,
    in_rs, ws_rs, x_rs, w_rs, wo_rs, pk_rs, pm_rs, st_rs, stz_rs, prev_rs, ap_rs, ad_rs, rs_rs,
    x_ss, xf_ss, w_ss, wf_ss, wo_ss, wof_ss, pk_ss, pm_ss, st_ss, stz_ss, prev_ss,
    ap_ss, ad_ss, apf_ss, adf_ss, rs_ss,
):
    sp, tp = lax.axis_index("sp"), lax.axis_index("tp")
    z, y = lax.div(sp, 4), lax.rem(sp, 4)
    x, c = lax.div(tp, 2), lax.rem(tp, 2)
    kh = lax.div(y, 2)
    yodd = lax.rem(y, 2)
    home = c == kh
    away = jnp.logical_not(home)

    def mod4(a):
        return lax.rem(a + 8, 4)

    def dev(zz, yy, xx, cc):
        return (4 * zz + yy, 2 * xx + cc)

    zp, zm, z2 = mod4(z + 1), mod4(z - 1), mod4(z + 2)
    yp, ym = mod4(y + 1), mod4(y - 1)
    xp, xm, x2 = mod4(x + 1), mod4(x - 1), mod4(x + 2)
    me_z, me_y, me_x = z, y, x
    partner = dev(z, y, x, 1 - c)

    ends = []

    def remote(src, dst, ssem, rsem, to, cond=None):
        def make():
            return pltpu.make_async_remote_copy(
                src_ref=src, dst_ref=dst, send_sem=ssem, recv_sem=rsem,
                device_id=to, device_id_type=MESH,
            )

        if cond is None:
            make().start()
            ends.append(lambda: make().wait_send())
        else:
            @pl.when(cond)
            def _():
                make().start()

            def end():
                @pl.when(cond)
                def _():
                    make().wait_send()

            ends.append(end)

    def arrived(ref, sem):
        pltpu.make_async_copy(ref, ref, sem).wait()

    loads = [
        (hld_in, hld_v), (dlb_in, dlb_v), (wlb_in, wlb_v), (factor_in, factor_v),
        (offset_in, offset_v), (pscale_in, pscale_v), (gain_in, gain_v), (hng_in, hng_v),
        (dw_in, rates_v.at[pl.ds(0, 16), :]), (sw_in, rates_v.at[pl.ds(16, 16), :]),
    ]
    for i, (src, dst) in enumerate(loads):
        pltpu.make_async_copy(src, dst, in_rs.at[i]).start()

    barrier = pltpu.get_barrier_semaphore()
    peers = [partner]
    for d in (1, 2, 3):
        for cc in (0, 1):
            peers.append(dev(mod4(z + d), y, x, cc))
            peers.append(dev(z, mod4(y + d), x, cc))
            peers.append(dev(z, y, mod4(x + d), cc))
    for to in peers:
        pl.semaphore_signal(barrier, inc=1, device_id=to, device_id_type=MESH)
    pl.semaphore_wait(barrier, len(peers))

    def xslot(yy, xx, u, quarter=None):
        start, size = 128 * (u % 2), 128
        if quarter is not None:
            start, size = start + 64 * quarter, 64
        return xbuf.at[2 * xx + u // 2, pl.ds(256 * lax.rem(yy, 2) + start, size), :]

    def xsem(yy, xx, u):
        return x_rs.at[16 * lax.rem(yy, 2) + 4 * xx + u]

    def wslot(zz, yy, r):
        return wbuf.at[2 * (4 * zz + yy) + r, :, pl.ds(0, 640)]

    def wsem(zz, yy, r):
        return w_rs.at[2 * (4 * zz + yy) + r]

    def woslot(zz, yy, cc, half=None):
        block = wo.at[zz, 2 * lax.rem(yy, 2) + cc]
        return block if half is None else block.at[pl.ds(256 * half, 256), :]

    def wosem(zz, yy, cc):
        return wo_rs.at[4 * zz + 2 * lax.rem(yy, 2) + cc]

    def own_x(half):
        src = x_in.at[pl.ds(128 * half, 128), :]
        dst = xbuf.at[tp, pl.ds(256 * yodd + 128 * half, 128), :]
        return src, dst, x_rs.at[16 * yodd + 2 * tp + half]

    def own_x_along_y(half, cond=None):
        src, dst, sem = own_x(half)
        for i, yy in enumerate((yp, ym)):
            at = 6 + 2 * half + i
            remote(src, dst, x_ss.at[at], sem, dev(z, yy, x, kh), cond)

    for half in (1, 0):
        src, dst, sem = own_x(half)
        for i, xx in enumerate((xp, xm)):
            remote(src, dst, x_ss.at[3 * half + i], sem, dev(z, y, xx, kh))
        remote(src, dst, x_ss.at[3 * half + 2], sem, partner, away)

        @pl.when(home)
        def _(src=src, dst=dst, sem=sem):
            pltpu.make_async_copy(src, dst, sem).start()

    own_x_along_y(0)
    own_x_along_y(1, c == 0)

    def both(p, q):
        return jnp.logical_and(p, q)

    for j in (0, 1):
        same = yodd == j
        for r in (0, 1):
            far = dev(z, yp if r == 0 else ym, x, r)
            for n, ref in enumerate((wp_in, wq_in, wk_in, wv_in, wg_in)):
                src = ref.at[pl.ds(128 * r, 128), pl.ds(128 * j, 128)]
                dst = w_stage.at[:, pl.ds(128 * n, 128)]
                remote(src, dst, w_ss.at[10 * j + 5 * r + n], ws_rs.at[0], far, both(away, same))
    for j in (0, 1):
        same = yodd == j
        head_y = 2 * c + j
        for r in (0, 1):
            here = both(both(home, same), c == r)
            direct = jnp.logical_not(jnp.logical_or(here, both(away, same)))
            for n, ref in enumerate((wp_in, wq_in, wk_in, wv_in, wg_in)):
                src = ref.at[pl.ds(128 * r, 128), pl.ds(128 * j, 128)]
                dst = wbuf.at[2 * sp + r, :, pl.ds(128 * n, 128)]
                remote(
                    src, dst, w_ss.at[20 + 10 * j + 5 * r + n], wsem(z, y, r),
                    dev(z, head_y, x, r), direct,
                )

                @pl.when(here)
                def _(src=src, dst=dst, r=r):
                    pltpu.make_async_copy(src, dst, wsem(z, y, r)).start()

    wo_own = wo.at[z, 2 * yodd + c]
    own_sem = wo_rs.at[4 * z + 2 * yodd + c]

    def own_wo(tos, at):
        for half, ref in enumerate((op_in, od_in)):
            part = wo_own.at[pl.ds(256 * half, 256), :]
            for i, to in enumerate(tos):
                remote(ref, part, wo_ss.at[at + 2 * half + i], own_sem, to)

    own_wo((dev(zp, y, x, kh), dev(zm, y, x, kh)), 0)
    for half, ref in enumerate((op_in, od_in)):
        part = wo_own.at[pl.ds(256 * half, 256), :]
        remote(ref, part, wo_ss.at[8 + half], own_sem, partner, away)

        @pl.when(home)
        def _(ref=ref, part=part):
            pltpu.make_async_copy(ref, part, own_sem).start()

    for i, (src, dst) in enumerate(loads):
        pltpu.make_async_copy(src, dst, in_rs.at[i]).wait()
    pk_src[0:2, :] = factor_v[...]
    pk_src[2:4, :] = offset_v[...]
    for j in (0, 1):
        for at, ref in ((4, hld_v), (6, dlb_v), (8, wlb_v)):
            pk_src[at + j : at + j + 1, :] = jnp.broadcast_to(ref[0:1, j : j + 1], (1, 256))
    pk_src[10:11, :] = pscale_v[...]
    for j in (0, 1):
        head_y = 2 * c + j
        self_here = jnp.logical_and(head_y == y, home)
        remote(
            pk_src, packb.at[yodd], pk_ss.at[j], pk_rs.at[yodd], dev(z, head_y, x, kh),
            jnp.logical_not(self_here),
        )

        @pl.when(self_here)
        def _():
            packb[yodd] = pk_src[...]

    remote(pm_in.at[yodd], pmb, pm_ss.at[0], pm_rs.at[0], partner, home)

    @pl.when(home)
    def _():
        pltpu.make_async_copy(pm_in.at[yodd], pmb, pm_rs.at[0]).start()

    def w_first(d, n):
        yy = mod4(me_y + d)
        slot = wslot(me_z, yy, c)
        arrived(slot, wsem(me_z, yy, c))
        remote(slot, slot, wf_ss.at[n], wsem(me_z, yy, c), dev(zp, y, x, c))
        remote(slot, slot, wf_ss.at[n + 1], wsem(me_z, yy, c), dev(zm, y, x, c))
        remote(slot, slot, wf_ss.at[n + 2], wsem(me_z, yy, c), partner)

    def w_later(zz, d, n, to_z=None):
        yy = mod4(me_y + d)
        slot = wslot(zz, yy, c)
        arrived(slot, wsem(zz, yy, c))
        if to_z is not None:
            remote(slot, slot, wf_ss.at[n + 1], wsem(zz, yy, c), dev(to_z, y, x, c))
        remote(slot, slot, wf_ss.at[n], wsem(zz, yy, c), partner)

    yn = 2 * c + 1 - yodd
    yo = 2 * c + yodd
    from_below = mod4(yn + 1) == y
    relay_half = jnp.where(from_below, 0, 1)
    y_next = jnp.where(from_below, yp, ym)
    xf_n = iter(range(64))
    wof_n = iter(range(64))

    def wait_if(cond, slot, sem):
        if cond is None:
            arrived(slot, sem)
        else:
            @pl.when(cond)
            def _():
                arrived(slot, sem)

    def x_pass(yy, xx, u, tos, relay=None, cond=None):
        slot, sem = xslot(yy, xx, u), xsem(yy, xx, u)
        wait_if(cond, slot, sem)
        for to in tos:
            remote(slot, slot, xf_ss.at[next(xf_n)], sem, to, cond)
        if relay is not None:
            half, to = relay
            part = xslot(yy, xx, u, half)
            remote(part, part, xf_ss.at[next(xf_n)], sem, to, cond)

    def wo_pass(zz, yy, cc, tos, relay=None, cond=None):
        slot, sem = woslot(zz, yy, cc), wosem(zz, yy, cc)
        wait_if(cond, slot, sem)
        for to in tos:
            remote(slot, slot, wof_ss.at[next(wof_n)], sem, to, cond)
        if relay is not None:
            half, to = relay
            part = woslot(zz, yy, cc, half)
            remote(part, part, wof_ss.at[next(wof_n)], sem, to, cond)

    FIRST_Y, FIRST_X = (0, 1, 2), (3,)
    x_ring = (dev(z, y, xp, c), dev(z, y, xm, c))
    y_ring = (dev(z, yp, x, c), dev(z, ym, x, c))
    z_ring = (dev(zp, y, x, c), dev(zm, y, x, c))
    y_relay = (relay_half, dev(z, y_next, x, c))

    yf = jnp.where(home, yo, yn)
    yl = jnp.where(home, yn, yo)

    def fill(i, carry):
        rows = pl.ds(pl.multiple_of(512 * i, 512), 512)
        both_cols = dot(rates_v[:, rows], pick, ((0,), (0,))).astype(BF16)
        wbuf[pl.ds(4 * i, 4), :, 640:768] = both_cols.reshape(4, 128, 128)
        return carry

    head = 4 * x + y
    row32, col32 = iota((32, 128), 0), iota((32, 128), 1)
    pick = jnp.logical_or(
        jnp.logical_and(row32 == head, col32 == 0),
        jnp.logical_and(row32 == head + 16, col32 == 1),
    ).astype(BF16)

    def project(i):
        gain = gain_f[pl.ds(i, 1), :]
        for b in range(4):
            rows = slice(128 * b, 128 * b + 128)
            v = xbuf[i, rows, :].astype(F32)
            sq = v * v
            ssq[rows, :] += (
                (sq[:, 0:128] + sq[:, 128:256]) + (sq[:, 256:384] + sq[:, 384:512])
            )
            xg[rows, :] = (v * gain).astype(BF16)
        acc[...] += dot(xg[...], wbuf[pl.ds(4 * i, 4)].reshape(512, 768))

    w_first(0, 0)
    for u in FIRST_X:
        x_pass(y, xm, u, y_ring, (0, x_ring[0]), home)
        x_pass(y, xp, u, y_ring, (1, x_ring[1]), home)
    for u in FIRST_Y:
        x_pass(yn, x, u, x_ring, y_relay)
    arrived(w_stage, ws_rs.at[0])
    stage_from = jnp.where(c == 0, ym, yp)
    stage_to = jnp.where(c == 0, yp, ym)
    stage_dst = wbuf.at[2 * (4 * z + stage_from) + c, :, pl.ds(0, 640)]
    remote(w_stage, stage_dst, w_ss.at[40], wsem(z, stage_from, c), dev(z, stage_to, x, c))
    for u in FIRST_Y:
        x_pass(y, xm, u, (), (0, x_ring[0]), home)
        x_pass(y, xp, u, (), (1, x_ring[1]), home)
    w_first(1, 3)
    w_first(3, 6)
    own_x_along_y(1, c == 1)
    for u in FIRST_Y:
        x_pass(yo, x, u, x_ring, None, away)
    for u in FIRST_Y:
        x_pass(yn, xm, u, (), (0, x_ring[0]))
        x_pass(yn, xp, u, (), (1, x_ring[1]))
    for u in FIRST_X:
        x_pass(yn, x, u, (), y_relay)
    lax.fori_loop(0, 8, fill, 0)
    gain_f[...] = gain_v[...].astype(F32)
    ssq[...] = jnp.zeros_like(ssq)
    acc[...] = jnp.zeros_like(acc)
    w_first(2, 9)
    own_wo((dev(z, yp, x, kh), dev(z, ym, x, kh)), 4)
    for u in FIRST_X:
        x_pass(y, x2, u, y_ring, None, home)
        x_pass(yn, xm, u, (), y_relay)
        x_pass(yn, xp, u, (), y_relay)
    n = 12
    for d in (0, 1):
        w_later(zm, d, n, zp if d in (0, 2) else None)
        w_later(zp, d, n + 2, zm if d in (1, 3) else None)
        n += 4
    for u in FIRST_Y:
        x_pass(yo, xm, u, (), (0, x_ring[0]), away)
        x_pass(yo, xp, u, (), (1, x_ring[1]), away)
    wo_pass(zm, y, 0, y_ring, (0, z_ring[0]), home)
    wo_pass(zp, y, 0, y_ring, (1, z_ring[1]), home)
    for d in (3, 2):
        w_later(zm, d, n, zp if d in (0, 2) else None)
        w_later(zp, d, n + 2, zm if d in (1, 3) else None)
        n += 4
    for u in FIRST_X:
        x_pass(yn, x2, u, (), y_relay)

    for u in FIRST_X:
        wait_if(home, xslot(y, x, u), xsem(y, x, u))
        for xx in (x, xm, xp):
            wait_if(away, xslot(yo, xx, u), xsem(yo, xx, u))
    for u in FIRST_Y:
        wait_if(home, xslot(y, x, u), xsem(y, x, u))
    for zz in (z, zp, zm):
        for d in (0, 1, 2, 3):
            yy = mod4(y + d)
            arrived(wslot(zz, yy, 1 - c), wsem(zz, yy, 1 - c))
    gap = mod4(x - z)
    e0 = jnp.where(gap == 2, xp, x)
    e1 = jnp.where(gap == 2, xm, jnp.where(gap == 0, xp, z))
    for i in (e0, e1):
        lax.fori_loop(2 * i, 2 * i + 2, lambda k, carry: (project(k), carry)[1], 0)

    wo_pass(z, yn, 1, z_ring, y_relay)
    for d in (0, 1, 3, 2):
        w_later(z2, d, n)
        n += 1

    for yy in (yn, yo):
        for u in FIRST_Y:
            arrived(xslot(yy, x2, u), xsem(yy, x2, u))
    for u in FIRST_X:
        wait_if(away, xslot(yo, x2, u), xsem(yo, x2, u))
    for d in (0, 1, 2, 3):
        yy = mod4(y + d)
        arrived(wslot(z2, yy, 1 - c), wsem(z2, yy, 1 - c))
    l0 = jnp.where(gap == 2, x, jnp.where(gap == 0, xm, x2))
    l1 = jnp.where(gap == 2, z, jnp.where(gap == 0, x2, mod4(z + 2)))

    for i in (l0, l1):
        lax.fori_loop(2 * i, 2 * i + 2, lambda k, carry: (project(k), carry)[1], 0)

    for b in (0, 1):
        @pl.when(jnp.logical_or(away, yodd != b))
        def _(b=b):
            arrived(packb.at[b], pk_rs.at[b])
    arrived(pmb, pm_rs.at[0])

    ii, jj = iota((256, 256), 0), iota((256, 256), 1)
    diff = jnp.bitwise_xor(ii, jj)
    lower = ii > jj
    causal = ii >= jj
    upto = (ii <= jj).astype(F32)
    eye = (ii == jj).astype(F32)

    def row_scale(b):
        total = jnp.sum(ssq[256 * b : 256 * b + 256, :], axis=-1, keepdims=True)
        return lax.rsqrt(total * (1.0 / 4096.0) + EPS)

    scale = [row_scale(0), row_scale(1)]

    for b in (0, 1):
        pad[16 + 256 * b : 272 + 256 * b, :] = acc[256 * b : 256 * b + 256, 0:128] * scale[b]
    prev_src[...] = pad[512:528, :].astype(BF16)
    prev_to = dev(jnp.where(c == 0, z, zp), y, x, 1 - c)
    last = jnp.logical_and(z == 3, c == 1)
    first = jnp.logical_and(z == 0, c == 0)
    prev_dst = ap.at[pl.ds(256, 16), pl.ds(0, 128)]
    remote(prev_src, prev_dst, prev_ss.at[0], prev_rs.at[0], prev_to, jnp.logical_not(last))

    heads = []
    for b in (0, 1):
        rows = slice(256 * b, 256 * b + 256)
        s = scale[b]
        q = unit(silu(acc[rows, 128:256] * s)) * HD ** (-0.5)
        k = unit(silu(acc[rows, 256:384] * s))
        v = silu(acc[rows, 384:512] * s)
        rate = acc[rows, 640:768] * s
        table = packb[b]
        of = lambda r: jnp.where(yodd == 0, table[r : r + 1, :], table[r + 1 : r + 2, :])
        factor, offset, hld, dlb, wlb = (of(r) for r in (0, 2, 4, 6, 8))
        pre = rate.T[0:1, :] + dlb
        soft = jnp.maximum(pre, 0.0) + jnp.log1p(jnp.exp(-jnp.abs(pre)))
        log_decay = -jnp.exp(hld) * soft * factor + offset
        run_row = dot(jnp.broadcast_to(log_decay, (8, 256)), upto, precision=HIGHEST)[0:1, :]
        run = jnp.broadcast_to(run_row, (128, 256)).T
        beta = jax.nn.sigmoid(rate[:, 1:2] + wlb[:, 0:1])
        spread = jnp.concatenate([run, run], axis=1) - run_row
        decay = jnp.where(causal, jnp.exp(jnp.where(causal, spread, 0.0)), 0.0)
        k16, q16 = k.astype(BF16), q.astype(BF16)
        low = jnp.where(lower, dot(k16, k16, ((1,), (1,))) * (decay * beta), 0.0)
        scores = (dot(q16, k16, ((1,), (1,))) * decay).astype(BF16)
        inverse = eye - jnp.where(diff == 1, low, 0.0)
        grown = jnp.exp(run)
        kb = k * beta
        low_s[b] = low
        inv_s[b] = inverse
        heads.append(dict(q=q, k=k, v=v, scores=scores, run=run, grown=grown, kb=kb, beta=beta))

    wo_pass(z, yo, 1, z_ring, None, away)
    wo_pass(z2, y, 0, y_ring, None, home)
    wo_pass(z, yn, 0, (), y_relay)
    for level in range(1, 8):
        mask = jnp.right_shift(diff, level) == 1
        mids = []
        for b in (0, 1):
            off = jnp.where(mask, low_s[b], 0.0).astype(BF16)
            mids.append(dot(off, inv_s[b].astype(BF16)).astype(BF16))
        for b, mid in enumerate(mids):
            inv_s[b] = inv_s[b] - dot(inv_s[b].astype(BF16), mid)

    maps = []
    for b, h in enumerate(heads):
        rows = slice(256 * b, 256 * b + 256)
        rhs = jnp.concatenate([h["v"] * h["beta"], h["kb"] * h["grown"]], axis=1)
        uw = rhs + dot((inv_s[b] - eye).astype(BF16), rhs.astype(BF16))
        uw16 = uw.astype(BF16)
        both = dot(h["scores"], uw16)
        o0[rows, :] = both[:, 0:128]
        pmx[rows, :] = (h["q"] * h["grown"] - both[:, 128:256]).astype(BF16)
        last_run = h["run"][255:256, :]
        kd = (h["k"] * jnp.exp(last_run - h["run"])).astype(BF16)
        ku = dot(kd, uw16, ((0,), (0,)))
        keep = jnp.exp(last_run)
        maps.append((keep, ku[:, 128:256].astype(BF16), ku[:, 0:128]))

    eye128 = (iota((128, 128), 0) == iota((128, 128), 1)).astype(F32)
    keep0, kw0, b0 = maps[0]
    keep1, kw1, b1 = maps[1]
    m0 = eye128 * keep0 - kw0.astype(F32)
    kw0_s[...] = kw0
    b0_s[...] = b0
    keep_s[0:1, :] = keep0
    first_map = jnp.concatenate([m0, b0], axis=1)
    keep1w = jnp.concatenate([keep1, keep1], axis=1)
    core_map = keep1w * first_map - dot(kw1, first_map.astype(BF16))
    core_map = core_map + jnp.concatenate([jnp.zeros_like(b1), b1], axis=1)
    stc[c] = core_map.astype(BF16)
    remote(stc.at[c], stc.at[c], st_ss.at[0], st_rs.at[c], partner)
    arrived(stc.at[1 - c], st_rs.at[1 - c])
    one = stc[1]
    chip_map = dot(one[:, 0:128], stc[0])
    chip_map = chip_map + jnp.concatenate([jnp.zeros_like(b1), one[:, 128:256].astype(F32)], axis=1)
    stz_src[...] = chip_map.astype(BF16)
    for d in (1, 2, 3):
        remote(
            stz_src, stz.at[z], stz_ss.at[d - 1], stz_rs.at[z],
            dev(mod4(z + d), y, x, c), z + d <= 3,
        )

    for yy in (yf, yl):
        wo_pass(zm, yy, 1, (), (0, z_ring[0]))
        wo_pass(zp, yy, 1, (), (1, z_ring[1]))
    for zz in (zm, zp):
        wo_pass(zz, yn, 0, (), y_relay)

    @pl.when(first)
    def _():
        pad[0:16, :] = jnp.zeros((16, 128), F32)

    @pl.when(jnp.logical_not(first))
    def _():
        arrived(prev_dst, prev_rs.at[0])
        pad[0:16, :] = ap[256:272, 0:128].astype(F32)

    window = jnp.left_shift(2, y)
    base = 512 * (2 * z + c)
    for b in (0, 1):
        at = 256 * b
        sums = pad[16 + at : 272 + at, :]
        here = sums
        for lag in range(1, 16):
            part = pad[16 + at - lag : 272 + at - lag, :]
            sums = sums + part * jnp.where(lag < window, 1.0, 0.0)
        counts = jnp.minimum(base + at + iota((256, 128), 0) + 1, window).astype(F32)
        pooled = (sums / counts - here).astype(BF16)
        row = packb[b]
        pscale = jnp.where(yodd == 0, row[10:11, 0:128], row[10:11, 128:256])
        pool_src[at : at + 256, :] = (dot(pooled, pmb[...]) * pscale).astype(BF16)

    def spread_out(src, dst, rsem, ssem):
        cols = pl.ds(128 * y, 128)

        @pl.when(home)
        def _():
            dst[0:256, cols] = src[pl.ds(256 * yodd, 256), :]

        for j in (0, 1):
            to_y = 2 * c + j
            here = to_y == y
            rows = pl.ds(256 * j, 256)
            remote(
                src.at[rows, :], dst.at[pl.ds(0, 256), cols], ssem.at[3 * j],
                rsem.at[y], partner, here,
            )
            for r in (0, 1):
                remote(
                    src.at[pl.ds(256 * j + 128 * r, 128), :],
                    dst.at[pl.ds(128 * r, 128), cols],
                    ssem.at[3 * j + 1 + r], rsem.at[y], dev(z, to_y, x, r),
                    jnp.logical_not(here),
                )

    def gather_in(dst, rsem, fsem):
        for i, d in enumerate((1, 3, 2)):
            yy = mod4(me_y + d)
            part = dst.at[pl.ds(128 * c, 128), pl.ds(128 * yy, 128)]
            arrived(part, rsem.at[yy])
            remote(part, part, fsem.at[i], rsem.at[4 + yy], partner)
        for d in (1, 3, 2):
            yy = mod4(me_y + d)
            part = dst.at[pl.ds(128 * (1 - c), 128), pl.ds(128 * yy, 128)]
            arrived(part, rsem.at[4 + yy])

        @pl.when(away)
        def _():
            arrived(dst.at[pl.ds(0, 256), pl.ds(128 * me_y, 128)], rsem.at[me_y])

    spread_out(pool_src, ap, ap_rs, ap_ss)

    state_s[...] = jnp.zeros((128, 128), F32)

    def absorb(part):
        moved = dot(part[:, 0:128], state_s[...].astype(BF16))
        state_s[...] = moved + part[:, 128:256].astype(F32)

    for i in (0, 1, 2):
        @pl.when(i < z)
        def _(i=i):
            arrived(stz.at[i], stz_rs.at[i])
            absorb(stz[i])

    @pl.when(c == 1)
    def _():
        absorb(stc[0])

    hng = hng_v[...]
    for b in (0, 1):
        rows = slice(256 * b, 256 * b + 256)
        s16 = state_s[...].astype(BF16)
        o = o0[rows, :] + dot(pmx[rows, :], s16)
        gate = silu(acc[rows, 512:640] * row_scale(b))
        norm = lax.rsqrt(jnp.mean(o * o, axis=-1, keepdims=True) + EPS)
        delta_src[rows, :] = (o * norm * hng * gate).astype(BF16)
        if b == 0:
            state_s[...] = keep_s[0:1, :] * state_s[...] - dot(kw0_s[...], s16) + b0_s[...]

    spread_out(delta_src, ad, ad_rs, ad_ss)

    wo_pass(z2, yn, 0, (), y_relay)
    for zz in (z, zm, zp, z2):
        wait_if(away, woslot(zz, yo, 0), wosem(zz, yo, 0))
    wait_if(home, woslot(z, y, 0), wosem(z, y, 0))
    wait_if(home, woslot(z, y, 1), wosem(z, y, 1))
    for yy in (yn, yo):
        arrived(woslot(z2, yy, 1), wosem(z2, yy, 1))

    gather_in(ap, ap_rs, apf_ss)
    gather_in(ad, ad_rs, adf_ss)

    def piece(zz):
        halves = []
        for j in (0, 1):
            part = None
            for cc in (0, 1):
                cols = slice(256 * cc, 256 * cc + 256)
                term = dot(ap[0:256, cols], wo[zz, 2 * j + cc, 0:256, :])
                term = term + dot(ad[0:256, cols], wo[zz, 2 * j + cc, 256:512, :])
                part = term if part is None else part + term
            halves.append(part)
        return jnp.concatenate(halves, axis=1)

    top, bottom = pl.ds(0, 128), pl.ds(128, 128)
    to_p, to_m = dev(z, y, xp, c), dev(z, y, xm, c)
    rs2[...] = piece(x2).astype(BF16)
    remote(rs2.at[top, :], rl.at[0], rs_ss.at[0], rs_rs.at[0], to_p)
    remote(rs2.at[bottom, :], rl.at[1], rs_ss.at[1], rs_rs.at[1], to_m)
    up_s[...] = piece(xp)
    rsp[128:256, :] = up_s[128:256, :].astype(BF16)
    remote(rsp.at[bottom, :], rin.at[0, bottom, :], rs_ss.at[2], rs_rs.at[2], to_p)
    down_s[...] = piece(xm)
    rsm[0:128, :] = down_s[0:128, :].astype(BF16)
    remote(rsm.at[top, :], rin.at[1, top, :], rs_ss.at[3], rs_rs.at[3], to_m)
    arrived(rl.at[0], rs_rs.at[0])
    rsp[0:128, :] = (up_s[0:128, :] + rl[0].astype(F32)).astype(BF16)
    remote(rsp.at[top, :], rin.at[0, top, :], rs_ss.at[4], rs_rs.at[4], to_p)
    arrived(rl.at[1], rs_rs.at[1])
    rsm[128:256, :] = (down_s[128:256, :] + rl[1].astype(F32)).astype(BF16)
    remote(rsm.at[bottom, :], rin.at[1, bottom, :], rs_ss.at[5], rs_rs.at[5], to_m)
    mine = piece(x)
    arrived(rin.at[0, bottom, :], rs_rs.at[2])
    arrived(rin.at[1, top, :], rs_rs.at[3])
    arrived(rin.at[0, top, :], rs_rs.at[4])
    arrived(rin.at[1, bottom, :], rs_rs.at[5])
    out_ref[...] = (mine + rin[0].astype(F32) + rin[1].astype(F32)).astype(BF16)

    for end in ends:
        end()


def per_device(
    inputs, input_norm_gain, pooling_input_weight, query_weight, key_weight,
    value_weight, gate_weight, decay_weight, strength_weight, pooling_group_map,
    pooling_scale, head_log_decay, decay_logit_bias, write_logit_bias,
    decay_position_factor, decay_position_offset, head_norm_gain,
    pooling_output_weight, delta_output_weight,
):
    dma = pltpu.SemaphoreType.DMA
    vmem = pltpu.VMEM
    hbm = pl.BlockSpec(memory_space=pl.ANY)
    local = pl.BlockSpec(memory_space=pltpu.VMEM)
    return pl.pallas_call(
        kernel,
        out_shape=jax.ShapeDtypeStruct((256, 512), BF16),
        in_specs=[hbm] * 19,
        out_specs=local,
        scratch_shapes=[
            vmem((1, 2), F32),
            vmem((1, 2), F32),
            vmem((1, 2), F32),
            vmem((8, 512), BF16),
            vmem((2, 256), F32),
            vmem((2, 256), F32),
            vmem((1, 256), F32),
            vmem((1, 128), F32),
            vmem((32, 4096), BF16),
            vmem((8, 512, 512), BF16),
            vmem((32, 128, 768), BF16),
            vmem((4, 4, 512, 256), BF16),
            vmem((8, 512), F32),
            vmem((16, 256), F32),
            vmem((2, 16, 256), F32),
            vmem((128, 128), BF16),
            vmem((512, 512), BF16),
            vmem((512, 768), F32),
            vmem((512, 128), F32),
            vmem((128, 640), BF16),
            vmem((2, 128, 256), BF16),
            vmem((128, 256), BF16),
            vmem((4, 128, 256), BF16),
            vmem((528, 128), F32),
            vmem((512, 128), BF16),
            vmem((512, 128), BF16),
            vmem((16, 128), BF16),
            vmem((272, 512), BF16),
            vmem((256, 512), BF16),
            vmem((256, 512), BF16),
            vmem((256, 512), BF16),
            vmem((256, 512), BF16),
            vmem((2, 128, 512), BF16),
            vmem((2, 256, 512), BF16),
            vmem((512, 128), F32),
            vmem((512, 128), BF16),
            vmem((128, 128), BF16),
            vmem((128, 128), F32),
            vmem((8, 128), F32),
            vmem((2, 256, 256), F32),
            vmem((2, 256, 256), F32),
            vmem((256, 512), F32),
            vmem((256, 512), F32),
            vmem((128, 128), F32),
            dma((10,)), dma((1,)), dma((32,)), dma((32,)), dma((16,)), dma((2,)), dma((1,)), dma((2,)),
            dma((4,)), dma((1,)), dma((8,)), dma((8,)), dma((6,)),
            dma((10,)), dma((48,)), dma((41,)), dma((32,)), dma((10,)), dma((32,)),
            dma((2,)), dma((1,)), dma((1,)), dma((3,)), dma((1,)),
            dma((6,)), dma((6,)), dma((3,)), dma((3,)), dma((6,)),
        ],
        compiler_params=pltpu.CompilerParams(
            collective_id=0, has_side_effects=True, vmem_limit_bytes=60 * 1024 * 1024
        ),
    )(
        inputs, pooling_input_weight, query_weight, key_weight, value_weight,
        gate_weight, pooling_output_weight, delta_output_weight, pooling_group_map,
        head_log_decay[None], decay_logit_bias[None], write_logit_bias[None],
        input_norm_gain.reshape(8, 512), decay_position_factor.T, decay_position_offset.T,
        pooling_scale[None], head_norm_gain[None], decay_weight.T, strength_weight.T,
    )


def solution(mesh):
    rows, heads = P("sp", "tp"), P("tp")
    in_specs = (
        rows, P(), rows, rows, rows, rows, rows, P(), P(), P("tp", None, None),
        heads, heads, heads, heads, rows, rows, P(), P("tp", "sp"), P("tp", "sp"),
    )
    return jax.shard_map(
        per_device, mesh=mesh, in_specs=in_specs, out_specs=rows, check_vma=False
    )
```

```python
import functools

import jax
import jax.numpy as jnp
from jax import lax
from jax.experimental import pallas as pl
from jax.experimental.pallas import tpu as pltpu
from jax.sharding import PartitionSpec as P

MESH = pl.DeviceIdType.MESH
F32 = jnp.float32
BF16 = jnp.bfloat16
HD = 128
EPS = 1e-06
HIGHEST = lax.Precision.HIGHEST


SCHEDULE = (
    ("TY",), ("TX",), ("TW",), ("OZ",), ("XA", 0), ("XR", "h", 3, 1), ("XR", "h", 1, 1),
    ("W0", 0), ("XR", "h", 1, 2), ("XB", 3), ("TS",), ("XA", 1), ("XO", 0), ("OXY",), ("W0", 3),
    ("WL", 1, 0), ("W0", 1), ("XB", 1), ("ST",), ("XR", "n", 1, 1), ("XA", 2), ("TB",),
    ("FILL",), ("WL", 3, 0), ("XR", "n", 3, 1), ("XN", 3), ("XR", "a", 1, 0), ("XR", "h", 3, 2),
    ("WL", 1, 3), ("XN", 0), ("XB2",), ("XN", 1), ("WL", 3, 1), ("XR", "n", 3, 2), ("W0", 2),
    ("OY",), ("XO", 1), ("XR", "h", 3, 0), ("XR", "h", 1, 0), ("XO", 2), ("WT", 3), ("XN", 2),
    ("WL", 3, 3), ("WL", 1, 1), ("XR", "n", 1, 0), ("WL", 3, 2), ("OB", 1), ("XR", "a", 1, 1),
    ("XR", "a", 3, 1), ("XR", "n", 3, 0), ("WL", 1, 2), ("XR", "n", 1, 2), ("OB", 3),
    ("XR", "a", 1, 2), ("XR", "a", 3, 0), ("OR", "h", 1), ("WT", 0), ("XR", "a", 3, 2),
    ("EARLY",), ("WT", 1), ("OR", "h", 3), ("WT", 2), ("OA",), ("ON", 0), ("LATE",), ("heads",),
    ("level", 1), ("level", 2), ("OB2",), ("level", 3), ("level", 4), ("level", 5),
    ("level", 6), ("OO",), ("level", 7), ("maps",), ("join",), ("OR", "n", 1), ("OR", "n", 3),
    ("ON", 3), ("ON", 1), ("pool",), ("state",), ("OR", "a", 3), ("OR", "a", 1), ("ON", 2),
    ("finish",), ("gather",), ("WOALL",),
)


def dot(a, b, dims=((1,), (0,)), precision=None):
    return lax.dot_general(
        a, b, (dims, ((), ())), precision=precision, preferred_element_type=F32
    )


def iota(shape, dim):
    return lax.broadcasted_iota(jnp.int32, shape, dim)


def silu(a):
    return a * jax.nn.sigmoid(a)


def unit(a):
    return a * lax.rsqrt(jnp.sum(a * a, axis=-1, keepdims=True) + EPS)


def kernel(
    x_in, wp_in, wq_in, wk_in, wv_in, wg_in, op_in, od_in, pm_in,
    hld_in, dlb_in, wlb_in, gain_in, factor_in, offset_in, pscale_in, hng_in, dw_in, sw_in,
    out_ref,
    hld_v, dlb_v, wlb_v, gain_v, factor_v, offset_v, pscale_v, hng_v, rates_v,
    xbuf, wbuf, wo, gain_f, pk_src, packb, pmb, xg, acc, ssq,
    w_stage, stc, stz_src, stz, pad, pool_src, delta_src, prev_src, ap, ad,
    rs2, rsp, rsm, rl, rin, o0, pmx, kw0_s, b0_s, keep_s, low_s, inv_s, up_s, down_s, state_s,
    in_rs, ws_rs, x_rs, w_rs, wo_rs, pk_rs, pm_rs, st_rs, stz_rs, prev_rs, ap_rs, ad_rs, rs_rs,
    x_ss, xf_ss, w_ss, wf_ss, wo_ss, wof_ss, pk_ss, pm_ss, st_ss, stz_ss, prev_ss,
    ap_ss, ad_ss, apf_ss, adf_ss, rs_ss,
):
    sp, tp = lax.axis_index("sp"), lax.axis_index("tp")
    z, y = lax.div(sp, 4), lax.rem(sp, 4)
    x, c = lax.div(tp, 2), lax.rem(tp, 2)
    kh = lax.div(y, 2)
    yodd = lax.rem(y, 2)
    home = c == kh
    away = jnp.logical_not(home)

    def mod4(a):
        return lax.rem(a + 8, 4)

    def dev(zz, yy, xx, cc):
        return (4 * zz + yy, 2 * xx + cc)

    zp, zm, z2 = mod4(z + 1), mod4(z - 1), mod4(z + 2)
    yp, ym = mod4(y + 1), mod4(y - 1)
    xp, xm, x2 = mod4(x + 1), mod4(x - 1), mod4(x + 2)
    me_z, me_y, me_x = z, y, x
    partner = dev(z, y, x, 1 - c)

    ends = []

    def remote(src, dst, ssem, rsem, to, cond=None):
        def make():
            return pltpu.make_async_remote_copy(
                src_ref=src, dst_ref=dst, send_sem=ssem, recv_sem=rsem,
                device_id=to, device_id_type=MESH,
            )

        if cond is None:
            make().start()
            ends.append(lambda: make().wait_send())
        else:
            @pl.when(cond)
            def _():
                make().start()

            def end():
                @pl.when(cond)
                def _():
                    make().wait_send()

            ends.append(end)

    def arrived(ref, sem):
        pltpu.make_async_copy(ref, ref, sem).wait()

    loads = [
        (hld_in, hld_v), (dlb_in, dlb_v), (wlb_in, wlb_v), (factor_in, factor_v),
        (offset_in, offset_v), (pscale_in, pscale_v), (gain_in, gain_v), (hng_in, hng_v),
        (dw_in, rates_v.at[pl.ds(0, 16), :]), (sw_in, rates_v.at[pl.ds(16, 16), :]),
    ]
    for i, (src, dst) in enumerate(loads):
        pltpu.make_async_copy(src, dst, in_rs.at[i]).start()

    barrier = pltpu.get_barrier_semaphore()
    peers = [partner]
    for d in (1, 2, 3):
        for cc in (0, 1):
            peers.append(dev(mod4(z + d), y, x, cc))
            peers.append(dev(z, mod4(y + d), x, cc))
            peers.append(dev(z, y, mod4(x + d), cc))
    for to in peers:
        pl.semaphore_signal(barrier, inc=1, device_id=to, device_id_type=MESH)
    pl.semaphore_wait(barrier, len(peers))

    def xslot(yy, xx, u, quarter=None):
        start, size = 128 * (u % 2), 128
        if quarter is not None:
            start, size = start + 64 * quarter, 64
        return xbuf.at[2 * xx + u // 2, pl.ds(256 * lax.rem(yy, 2) + start, size), :]

    def xsem(yy, xx, u):
        return x_rs.at[16 * lax.rem(yy, 2) + 4 * xx + u]

    def wslot(zz, yy, r):
        return wbuf.at[2 * (4 * zz + yy) + r, :, pl.ds(0, 640)]

    def wsem(zz, yy, r):
        return w_rs.at[2 * (4 * zz + yy) + r]

    def woslot(zz, yy, cc, half=None):
        block = wo.at[zz, 2 * lax.rem(yy, 2) + cc]
        return block if half is None else block.at[pl.ds(256 * half, 256), :]

    def wosem(zz, yy, cc):
        return wo_rs.at[4 * zz + 2 * lax.rem(yy, 2) + cc]

    def own_x(half):
        src = x_in.at[pl.ds(128 * half, 128), :]
        dst = xbuf.at[tp, pl.ds(256 * yodd + 128 * half, 128), :]
        return src, dst, x_rs.at[16 * yodd + 2 * tp + half]

    def own_x_along_y(half, cond=None):
        src, dst, sem = own_x(half)
        for i, yy in enumerate((yp, ym)):
            at = 6 + 2 * half + i
            remote(src, dst, x_ss.at[at], sem, dev(z, yy, x, kh), cond)

    def both(p, q):
        return jnp.logical_and(p, q)

    wo_own = wo.at[z, 2 * yodd + c]
    own_sem = wo_rs.at[4 * z + 2 * yodd + c]

    def own_wo(tos, at):
        for half, ref in enumerate((op_in, od_in)):
            part = wo_own.at[pl.ds(256 * half, 256), :]
            for i, to in enumerate(tos):
                remote(ref, part, wo_ss.at[at + 2 * half + i], own_sem, to)

    yn = 2 * c + 1 - yodd
    yo = 2 * c + yodd
    from_below = mod4(yn + 1) == y
    relay_half = jnp.where(from_below, 0, 1)
    y_next = jnp.where(from_below, yp, ym)
    xf_n, wf_n, wof_n = iter(range(64)), iter(range(64)), iter(range(64))
    x_ring = (dev(z, y, xp, c), dev(z, y, xm, c))
    y_ring = (dev(z, yp, x, c), dev(z, ym, x, c))
    z_ring = (dev(zp, y, x, c), dev(zm, y, x, c))
    y_relay = (relay_half, dev(z, y_next, x, c))
    x_relay = {3: (0, x_ring[0]), 1: (1, x_ring[1])}
    z_relay = {3: (0, z_ring[0]), 1: (1, z_ring[1])}
    x_at, z_at = (x, xp, x2, xm), (z, zp, z2, zm)
    cases = {"n": (yn, None), "h": (yo, home), "a": (yo, away)}
    seen = set()

    def take(key, slot, sem, cond=None):
        if key in seen:
            return
        seen.add(key)
        if cond is None:
            arrived(slot, sem)
        else:
            @pl.when(cond)
            def _():
                arrived(slot, sem)

    def x_take(case, d, u):
        yy, cond = cases[case]
        take(("x", case, d, u), xslot(yy, x_at[d], u), xsem(yy, x_at[d], u), cond)

    def x_pass(case, d, u, tos, relay=None):
        x_take(case, d, u)
        yy, cond = cases[case]
        slot, sem = xslot(yy, x_at[d], u), xsem(yy, x_at[d], u)
        for to in tos:
            remote(slot, slot, xf_ss.at[next(xf_n)], sem, to, cond)
        if relay is not None:
            half, to = relay
            part = xslot(yy, x_at[d], u, half)
            remote(part, part, xf_ss.at[next(xf_n)], sem, to, cond)

    def o_take(case, d, cc):
        yy, cond = cases[case]
        take(("o", case, d, cc), woslot(z_at[d], yy, cc), wosem(z_at[d], yy, cc), cond)

    def o_pass(case, d, cc, tos, relay=None):
        o_take(case, d, cc)
        yy, cond = cases[case]
        slot, sem = woslot(z_at[d], yy, cc), wosem(z_at[d], yy, cc)
        for to in tos:
            remote(slot, slot, wof_ss.at[next(wof_n)], sem, to, cond)
        if relay is not None:
            half, to = relay
            part = woslot(z_at[d], yy, cc, half)
            remote(part, part, wof_ss.at[next(wof_n)], sem, to, cond)

    def w_take(d, e, r, tag):
        yy = mod4(me_y + e)
        take((tag, d, e), wslot(z_at[d], yy, r), wsem(z_at[d], yy, r))

    def w_pass(d, e, tos):
        w_take(d, e, c, "w")
        yy = mod4(me_y + e)
        slot, sem = wslot(z_at[d], yy, c), wsem(z_at[d], yy, c)
        for to in (*tos, partner):
            remote(slot, slot, wf_ss.at[next(wf_n)], sem, to)

    def fill(i, carry):
        rows = pl.ds(pl.multiple_of(512 * i, 512), 512)
        both_cols = dot(rates_v[:, rows], pick, ((0,), (0,))).astype(BF16)
        wbuf[pl.ds(4 * i, 4), :, 640:768] = both_cols.reshape(4, 128, 128)
        return carry

    head = 4 * x + y
    row32, col32 = iota((32, 128), 0), iota((32, 128), 1)
    pick = jnp.logical_or(
        jnp.logical_and(row32 == head, col32 == 0),
        jnp.logical_and(row32 == head + 16, col32 == 1),
    ).astype(BF16)

    def project(i):
        gains = [gain_f[pl.ds(4 * i + q, 1), :] for q in range(4)]
        gain = jnp.concatenate(gains, axis=1)
        for b in range(4):
            rows = slice(128 * b, 128 * b + 128)
            v = xbuf[i, rows, :].astype(F32)
            sq = v * v
            ssq[rows, :] += (
                (sq[:, 0:128] + sq[:, 128:256]) + (sq[:, 256:384] + sq[:, 384:512])
            )
            xg[rows, :] = (v * gain).astype(BF16)
        acc[...] += dot(xg[...], wbuf[pl.ds(4 * i, 4)].reshape(512, 768))

    ii, jj = iota((256, 256), 0), iota((256, 256), 1)
    diff = jnp.bitwise_xor(ii, jj)
    lower = ii > jj
    causal = ii >= jj
    upto = (ii <= jj).astype(F32)
    eye = (ii == jj).astype(F32)

    def row_scale(b):
        total = jnp.sum(ssq[256 * b : 256 * b + 256, :], axis=-1, keepdims=True)
        return lax.rsqrt(total * (1.0 / 4096.0) + EPS)

    prev_to = dev(jnp.where(c == 0, z, zp), y, x, 1 - c)
    last = jnp.logical_and(z == 3, c == 1)
    first = jnp.logical_and(z == 0, c == 0)
    prev_dst = ap.at[pl.ds(256, 16), pl.ds(0, 128)]
    heads = []
    maps = []

    def spread_out(src, dst, rsem, ssem):
        cols = pl.ds(128 * y, 128)

        @pl.when(home)
        def _():
            dst[0:256, cols] = src[pl.ds(256 * yodd, 256), :]

        for j in (0, 1):
            to_y = 2 * c + j
            here = to_y == y
            rows = pl.ds(256 * j, 256)
            remote(
                src.at[rows, :], dst.at[pl.ds(0, 256), cols], ssem.at[3 * j],
                rsem.at[y], partner, here,
            )
            for r in (0, 1):
                remote(
                    src.at[pl.ds(256 * j + 128 * r, 128), :],
                    dst.at[pl.ds(128 * r, 128), cols],
                    ssem.at[3 * j + 1 + r], rsem.at[y], dev(z, to_y, x, r),
                    jnp.logical_not(here),
                )

    def gather_in(dst, rsem, fsem):
        for i, d in enumerate((1, 3, 2)):
            yy = mod4(me_y + d)
            part = dst.at[pl.ds(128 * c, 128), pl.ds(128 * yy, 128)]
            arrived(part, rsem.at[yy])
            remote(part, part, fsem.at[i], rsem.at[4 + yy], partner)
        for d in (1, 3, 2):
            yy = mod4(me_y + d)
            part = dst.at[pl.ds(128 * (1 - c), 128), pl.ds(128 * yy, 128)]
            arrived(part, rsem.at[4 + yy])

        @pl.when(away)
        def _():
            arrived(dst.at[pl.ds(0, 256), pl.ds(128 * me_y, 128)], rsem.at[me_y])

    def t_x():
        for half in (1, 0):
            src, dst, sem = own_x(half)
            for i, xx in enumerate((xp, xm)):
                remote(src, dst, x_ss.at[3 * half + i], sem, dev(z, y, xx, kh))
            remote(src, dst, x_ss.at[3 * half + 2], sem, partner, away)

            @pl.when(home)
            def _(src=src, dst=dst, sem=sem):
                pltpu.make_async_copy(src, dst, sem).start()

    def t_y():
        own_x_along_y(0)
        own_x_along_y(1, c == 0)

    def t_s():
        for j in (0, 1):
            same = yodd == j
            for r in (0, 1):
                far = dev(z, yp if r == 0 else ym, x, r)
                for n, ref in enumerate((wp_in, wq_in, wk_in, wv_in, wg_in)):
                    src = ref.at[pl.ds(128 * r, 128), pl.ds(128 * j, 128)]
                    dst = w_stage.at[:, pl.ds(128 * n, 128)]
                    remote(src, dst, w_ss.at[10 * j + 5 * r + n], ws_rs.at[0], far, both(away, same))

    def t_w():
        for j in (0, 1):
            same = yodd == j
            head_y = 2 * c + j
            for r in (0, 1):
                here = both(both(home, same), c == r)
                direct = jnp.logical_not(jnp.logical_or(here, both(away, same)))
                for n, ref in enumerate((wp_in, wq_in, wk_in, wv_in, wg_in)):
                    src = ref.at[pl.ds(128 * r, 128), pl.ds(128 * j, 128)]
                    dst = wbuf.at[2 * sp + r, :, pl.ds(128 * n, 128)]
                    remote(
                        src, dst, w_ss.at[20 + 10 * j + 5 * r + n], wsem(z, y, r),
                        dev(z, head_y, x, r), direct,
                    )

                    @pl.when(here)
                    def _(src=src, dst=dst, r=r):
                        pltpu.make_async_copy(src, dst, wsem(z, y, r)).start()

        for half, ref in enumerate((op_in, od_in)):
            part = wo_own.at[pl.ds(256 * half, 256), :]
            remote(ref, part, wo_ss.at[8 + half], own_sem, partner, away)

            @pl.when(home)
            def _(ref=ref, part=part):
                pltpu.make_async_copy(ref, part, own_sem).start()

    def t_b():
        for i, (src, dst) in enumerate(loads):
            pltpu.make_async_copy(src, dst, in_rs.at[i]).wait()
        pk_src[0:2, :] = factor_v[...]
        pk_src[2:4, :] = offset_v[...]
        for j in (0, 1):
            for at, ref in ((4, hld_v), (6, dlb_v), (8, wlb_v)):
                pk_src[at + j : at + j + 1, :] = jnp.broadcast_to(ref[0:1, j : j + 1], (1, 256))
        pk_src[10:11, :] = pscale_v[...]
        for j in (0, 1):
            head_y = 2 * c + j
            self_here = jnp.logical_and(head_y == y, home)
            remote(
                pk_src, packb.at[yodd], pk_ss.at[j], pk_rs.at[yodd], dev(z, head_y, x, kh),
                jnp.logical_not(self_here),
            )

            @pl.when(self_here)
            def _():
                packb[yodd] = pk_src[...]

        remote(pm_in.at[yodd], pmb, pm_ss.at[0], pm_rs.at[0], partner, home)

        @pl.when(home)
        def _():
            pltpu.make_async_copy(pm_in.at[yodd], pmb, pm_rs.at[0]).start()

    def stage():
        arrived(w_stage, ws_rs.at[0])
        stage_from = jnp.where(c == 0, ym, yp)
        stage_to = jnp.where(c == 0, yp, ym)
        stage_dst = wbuf.at[2 * (4 * z + stage_from) + c, :, pl.ds(0, 640)]
        remote(w_stage, stage_dst, w_ss.at[40], wsem(z, stage_from, c), dev(z, stage_to, x, c))

    def start_rates():
        lax.fori_loop(0, 8, fill, 0)
        gain_f[...] = gain_v[...].astype(F32)
        ssq[...] = jnp.zeros_like(ssq)
        acc[...] = jnp.zeros_like(acc)

    gap = mod4(x - z)

    def depth(parts, ds):
        for d in ds:
            for case in "nha":
                for u in range(4):
                    x_take(case, d, u)
            for e in (0, 1, 2, 3):
                w_take(d, e, c, "w")
                w_take(d, e, 1 - c, "p")
        for i in parts:
            lax.fori_loop(2 * i, 2 * i + 2, lambda k, carry: (project(k), carry)[1], 0)

    def early():
        first_part = jnp.where(gap == 2, xp, x)
        depth((first_part, jnp.where(gap == 2, xm, jnp.where(gap == 0, xp, z))), (0, 1, 3))

    def late():
        third = jnp.where(gap == 2, x, jnp.where(gap == 0, xm, x2))
        depth((third, jnp.where(gap == 2, z, jnp.where(gap == 0, x2, z2))), (2,))

    def delta_heads():
        for b in (0, 1):
            @pl.when(jnp.logical_or(away, yodd != b))
            def _(b=b):
                arrived(packb.at[b], pk_rs.at[b])
        arrived(pmb, pm_rs.at[0])

        scale = [row_scale(0), row_scale(1)]

        for b in (0, 1):
            pad[16 + 256 * b : 272 + 256 * b, :] = acc[256 * b : 256 * b + 256, 0:128] * scale[b]
        prev_src[...] = pad[512:528, :].astype(BF16)
        remote(prev_src, prev_dst, prev_ss.at[0], prev_rs.at[0], prev_to, jnp.logical_not(last))

        for b in (0, 1):
            rows = slice(256 * b, 256 * b + 256)
            s = scale[b]
            q = unit(silu(acc[rows, 128:256] * s)) * HD ** (-0.5)
            k = unit(silu(acc[rows, 256:384] * s))
            v = silu(acc[rows, 384:512] * s)
            rate = acc[rows, 640:768] * s
            table = packb[b]
            of = lambda r: jnp.where(yodd == 0, table[r : r + 1, :], table[r + 1 : r + 2, :])
            factor, offset, hld, dlb, wlb = (of(r) for r in (0, 2, 4, 6, 8))
            pre = rate.T[0:1, :] + dlb
            soft = jnp.maximum(pre, 0.0) + jnp.log1p(jnp.exp(-jnp.abs(pre)))
            log_decay = -jnp.exp(hld) * soft * factor + offset
            run_row = dot(jnp.broadcast_to(log_decay, (8, 256)), upto, precision=HIGHEST)[0:1, :]
            run = jnp.broadcast_to(run_row, (128, 256)).T
            beta = jax.nn.sigmoid(rate[:, 1:2] + wlb[:, 0:1])
            spread = jnp.concatenate([run, run], axis=1) - run_row
            decay = jnp.where(causal, jnp.exp(jnp.where(causal, spread, 0.0)), 0.0)
            k16, q16 = k.astype(BF16), q.astype(BF16)
            low = jnp.where(lower, dot(k16, k16, ((1,), (1,))) * (decay * beta), 0.0)
            scores = (dot(q16, k16, ((1,), (1,))) * decay).astype(BF16)
            inverse = eye - jnp.where(diff == 1, low, 0.0)
            grown = jnp.exp(run)
            kb = k * beta
            low_s[b] = low
            inv_s[b] = inverse
            heads.append(dict(q=q, k=k, v=v, scores=scores, run=run, grown=grown, kb=kb, beta=beta))

    def level_step(level):
        mask = jnp.right_shift(diff, level) == 1
        mids = []
        for b in (0, 1):
            off = jnp.where(mask, low_s[b], 0.0).astype(BF16)
            mids.append(dot(off, inv_s[b].astype(BF16)).astype(BF16))
        for b, mid in enumerate(mids):
            inv_s[b] = inv_s[b] - dot(inv_s[b].astype(BF16), mid)

    def delta_maps():
        for b, h in enumerate(heads):
            rows = slice(256 * b, 256 * b + 256)
            rhs = jnp.concatenate([h["v"] * h["beta"], h["kb"] * h["grown"]], axis=1)
            uw = rhs + dot((inv_s[b] - eye).astype(BF16), rhs.astype(BF16))
            uw16 = uw.astype(BF16)
            both = dot(h["scores"], uw16)
            o0[rows, :] = both[:, 0:128]
            pmx[rows, :] = (h["q"] * h["grown"] - both[:, 128:256]).astype(BF16)
            last_run = h["run"][255:256, :]
            kd = (h["k"] * jnp.exp(last_run - h["run"])).astype(BF16)
            ku = dot(kd, uw16, ((0,), (0,)))
            keep = jnp.exp(last_run)
            maps.append((keep, ku[:, 128:256].astype(BF16), ku[:, 0:128]))

        eye128 = (iota((128, 128), 0) == iota((128, 128), 1)).astype(F32)
        keep0, kw0, b0 = maps[0]
        keep1, kw1, b1 = maps[1]
        m0 = eye128 * keep0 - kw0.astype(F32)
        kw0_s[...] = kw0
        b0_s[...] = b0
        keep_s[0:1, :] = keep0
        first_map = jnp.concatenate([m0, b0], axis=1)
        keep1w = jnp.concatenate([keep1, keep1], axis=1)
        core_map = keep1w * first_map - dot(kw1, first_map.astype(BF16))
        core_map = core_map + jnp.concatenate([jnp.zeros_like(b1), b1], axis=1)
        stc[c] = core_map.astype(BF16)
        remote(stc.at[c], stc.at[c], st_ss.at[0], st_rs.at[c], partner)

    def join_maps():
        arrived(stc.at[1 - c], st_rs.at[1 - c])
        one = stc[1]
        chip_map = dot(one[:, 0:128], stc[0])
        chip_map = chip_map + jnp.concatenate([jnp.zeros((128, 128), F32), one[:, 128:256].astype(F32)], axis=1)
        stz_src[...] = chip_map.astype(BF16)
        for d in (1, 2, 3):
            remote(
                stz_src, stz.at[z], stz_ss.at[d - 1], stz_rs.at[z],
                dev(mod4(z + d), y, x, c), z + d <= 3,
            )

    def pool_part():
        @pl.when(first)
        def _():
            pad[0:16, :] = jnp.zeros((16, 128), F32)

        @pl.when(jnp.logical_not(first))
        def _():
            arrived(prev_dst, prev_rs.at[0])
            pad[0:16, :] = ap[256:272, 0:128].astype(F32)

        window = jnp.left_shift(2, y)
        base = 512 * (2 * z + c)
        for b in (0, 1):
            at = 256 * b
            sums = pad[16 + at : 272 + at, :]
            here = sums
            for lag in range(1, 16):
                part = pad[16 + at - lag : 272 + at - lag, :]
                sums = sums + part * jnp.where(lag < window, 1.0, 0.0)
            counts = jnp.minimum(base + at + iota((256, 128), 0) + 1, window).astype(F32)
            pooled = (sums / counts - here).astype(BF16)
            row = packb[b]
            pscale = jnp.where(yodd == 0, row[10:11, 0:128], row[10:11, 128:256])
            pool_src[at : at + 256, :] = (dot(pooled, pmb[...]) * pscale).astype(BF16)

        spread_out(pool_src, ap, ap_rs, ap_ss)

    def state_in():
        state_s[...] = jnp.zeros((128, 128), F32)

        def absorb(part):
            moved = dot(part[:, 0:128], state_s[...].astype(BF16))
            state_s[...] = moved + part[:, 128:256].astype(F32)

        for i in (0, 1, 2):
            @pl.when(i < z)
            def _(i=i):
                arrived(stz.at[i], stz_rs.at[i])
                absorb(stz[i])

        @pl.when(c == 1)
        def _():
            absorb(stc[0])

    def finish():
        hng = hng_v[...]
        for b in (0, 1):
            rows = slice(256 * b, 256 * b + 256)
            s16 = state_s[...].astype(BF16)
            o = o0[rows, :] + dot(pmx[rows, :], s16)
            gate = silu(acc[rows, 512:640] * row_scale(b))
            norm = lax.rsqrt(jnp.mean(o * o, axis=-1, keepdims=True) + EPS)
            delta_src[rows, :] = (o * norm * hng * gate).astype(BF16)
            if b == 0:
                state_s[...] = keep_s[0:1, :] * state_s[...] - dot(kw0_s[...], s16) + b0_s[...]

        spread_out(delta_src, ad, ad_rs, ad_ss)

    def gather_both():
        gather_in(ap, ap_rs, apf_ss)
        gather_in(ad, ad_rs, adf_ss)

    def rest_of_output_weights():
        for d in range(4):
            for case in "nha":
                for cc in (0, 1):
                    o_take(case, d, cc)

    ops = dict(
        TX=t_x, gather=gather_both, TY=t_y, TS=t_s, TW=t_w, TB=t_b, ST=stage, FILL=start_rates, EARLY=early,
        LATE=late, heads=delta_heads, level=level_step, maps=delta_maps, join=join_maps,
        pool=pool_part, state=state_in, finish=finish, WOALL=rest_of_output_weights,
        W0=lambda e: w_pass(0, e, z_ring),
        WL=lambda d, e: w_pass(d, e, (z_relay[d][1],) if (d == 3) == (e in (0, 2)) else ()),
        WT=lambda e: w_pass(2, e, ()),
        XA=lambda u: x_pass("n", 0, u, x_ring, y_relay),
        XO=lambda u: x_pass("a", 0, u, x_ring),
        XB=lambda d: x_pass("h", d, 3, y_ring, x_relay[d]),
        XB2=lambda: x_pass("h", 2, 3, y_ring),
        XN=lambda d: x_pass("n", d, 3, (), y_relay),
        XR=lambda case, d, u: x_pass(case, d, u, (), x_relay[d]),
        OXY=lambda: own_x_along_y(1, c == 1),
        OY=lambda: own_wo((dev(z, yp, x, kh), dev(z, ym, x, kh)), 4),
        OZ=lambda: own_wo((dev(zp, y, x, kh), dev(zm, y, x, kh)), 0),
        OA=lambda: o_pass("n", 0, 1, z_ring, y_relay),
        OO=lambda: o_pass("a", 0, 1, z_ring),
        OB=lambda d: o_pass("h", d, 0, y_ring, z_relay[d]),
        OB2=lambda: o_pass("h", 2, 0, y_ring),
        ON=lambda d: o_pass("n", d, 0, (), y_relay),
        OR=lambda case, d: o_pass(case, d, 1, (), z_relay[d]),
    )
    for name, *args in SCHEDULE:
        ops[name](*args)

    def piece(zz):
        halves = []
        for j in (0, 1):
            part = None
            for cc in (0, 1):
                cols = slice(256 * cc, 256 * cc + 256)
                term = dot(ap[0:256, cols], wo[zz, 2 * j + cc, 0:256, :])
                term = term + dot(ad[0:256, cols], wo[zz, 2 * j + cc, 256:512, :])
                part = term if part is None else part + term
            halves.append(part)
        return jnp.concatenate(halves, axis=1)

    top, bottom = pl.ds(0, 128), pl.ds(128, 128)
    to_p, to_m = dev(z, y, xp, c), dev(z, y, xm, c)
    rs2[...] = piece(x2).astype(BF16)
    remote(rs2.at[top, :], rl.at[0], rs_ss.at[0], rs_rs.at[0], to_p)
    remote(rs2.at[bottom, :], rl.at[1], rs_ss.at[1], rs_rs.at[1], to_m)
    up_s[...] = piece(xp)
    rsp[128:256, :] = up_s[128:256, :].astype(BF16)
    remote(rsp.at[bottom, :], rin.at[0, bottom, :], rs_ss.at[2], rs_rs.at[2], to_p)
    down_s[...] = piece(xm)
    rsm[0:128, :] = down_s[0:128, :].astype(BF16)
    remote(rsm.at[top, :], rin.at[1, top, :], rs_ss.at[3], rs_rs.at[3], to_m)
    arrived(rl.at[0], rs_rs.at[0])
    rsp[0:128, :] = (up_s[0:128, :] + rl[0].astype(F32)).astype(BF16)
    remote(rsp.at[top, :], rin.at[0, top, :], rs_ss.at[4], rs_rs.at[4], to_p)
    arrived(rl.at[1], rs_rs.at[1])
    rsm[128:256, :] = (down_s[128:256, :] + rl[1].astype(F32)).astype(BF16)
    remote(rsm.at[bottom, :], rin.at[1, bottom, :], rs_ss.at[5], rs_rs.at[5], to_m)
    mine = piece(x)
    arrived(rin.at[0, bottom, :], rs_rs.at[2])
    arrived(rin.at[1, top, :], rs_rs.at[3])
    arrived(rin.at[0, top, :], rs_rs.at[4])
    arrived(rin.at[1, bottom, :], rs_rs.at[5])
    out_ref[...] = (mine + rin[0].astype(F32) + rin[1].astype(F32)).astype(BF16)

    for end in ends:
        end()


def per_device(
    inputs, input_norm_gain, pooling_input_weight, query_weight, key_weight,
    value_weight, gate_weight, decay_weight, strength_weight, pooling_group_map,
    pooling_scale, head_log_decay, decay_logit_bias, write_logit_bias,
    decay_position_factor, decay_position_offset, head_norm_gain,
    pooling_output_weight, delta_output_weight,
):
    dma = pltpu.SemaphoreType.DMA
    vmem = pltpu.VMEM
    hbm = pl.BlockSpec(memory_space=pl.ANY)
    local = pl.BlockSpec(memory_space=pltpu.VMEM)
    return pl.pallas_call(
        kernel,
        out_shape=pltpu.VMEM((256, 512), BF16),
        in_specs=[hbm] * 19,
        out_specs=local,
        scratch_shapes=[
            vmem((1, 2), F32),
            vmem((1, 2), F32),
            vmem((1, 2), F32),
            vmem((32, 128), BF16),
            vmem((2, 256), F32),
            vmem((2, 256), F32),
            vmem((1, 256), F32),
            vmem((1, 128), F32),
            vmem((32, 4096), BF16),
            vmem((8, 512, 512), BF16),
            vmem((32, 128, 768), BF16),
            vmem((4, 4, 512, 256), BF16),
            vmem((32, 128), F32),
            vmem((16, 256), F32),
            vmem((2, 16, 256), F32),
            vmem((128, 128), BF16),
            vmem((512, 512), BF16),
            vmem((512, 768), F32),
            vmem((512, 128), F32),
            vmem((128, 640), BF16),
            vmem((2, 128, 256), BF16),
            vmem((128, 256), BF16),
            vmem((4, 128, 256), BF16),
            vmem((528, 128), F32),
            vmem((512, 128), BF16),
            vmem((512, 128), BF16),
            vmem((16, 128), BF16),
            vmem((272, 512), BF16),
            vmem((256, 512), BF16),
            vmem((256, 512), BF16),
            vmem((256, 512), BF16),
            vmem((256, 512), BF16),
            vmem((2, 128, 512), BF16),
            vmem((2, 256, 512), BF16),
            vmem((512, 128), F32),
            vmem((512, 128), BF16),
            vmem((128, 128), BF16),
            vmem((128, 128), F32),
            vmem((8, 128), F32),
            vmem((2, 256, 256), F32),
            vmem((2, 256, 256), F32),
            vmem((256, 512), F32),
            vmem((256, 512), F32),
            vmem((128, 128), F32),
            dma((10,)), dma((1,)), dma((32,)), dma((32,)), dma((16,)), dma((2,)), dma((1,)), dma((2,)),
            dma((4,)), dma((1,)), dma((8,)), dma((8,)), dma((6,)),
            dma((10,)), dma((48,)), dma((41,)), dma((32,)), dma((10,)), dma((32,)),
            dma((2,)), dma((1,)), dma((1,)), dma((3,)), dma((1,)),
            dma((6,)), dma((6,)), dma((3,)), dma((3,)), dma((6,)),
        ],
        compiler_params=pltpu.CompilerParams(
            collective_id=0, has_side_effects=True, vmem_limit_bytes=60 * 1024 * 1024
        ),
    )(
        inputs, pooling_input_weight, query_weight, key_weight, value_weight,
        gate_weight, pooling_output_weight, delta_output_weight, pooling_group_map,
        head_log_decay[None], decay_logit_bias[None], write_logit_bias[None],
        input_norm_gain.reshape(32, 128), decay_position_factor.T, decay_position_offset.T,
        pooling_scale[None], head_norm_gain[None], decay_weight.T, strength_weight.T,
    )


def solution(mesh):
    rows, heads = P("sp", "tp"), P("tp")
    in_specs = (
        rows, P(), rows, rows, rows, rows, rows, P(), P(), P("tp", None, None),
        heads, heads, heads, heads, rows, rows, P(), P("tp", "sp"), P("tp", "sp"),
    )
    return jax.shard_map(
        per_device, mesh=mesh, in_specs=in_specs, out_specs=rows, check_vma=False
    )
```

```python
import functools

import jax
import jax.numpy as jnp
from jax import lax
from jax.experimental import pallas as pl
from jax.experimental.pallas import tpu as pltpu
from jax.sharding import PartitionSpec as P

MESH = pl.DeviceIdType.MESH
F32 = jnp.float32
BF16 = jnp.bfloat16
HD = 128
EPS = 1e-06
PARTS = ((0, 128), (128, 128), (0, 128), (128, 128))
HIGHEST = lax.Precision.HIGHEST


SCHEDULE = (
    ("TX",), ("TY",), ("TW",), ("OZ",), ("XR", "h", 3, 1), ("XA", 0), ("W0", 0),
    ("XR", "h", 1, 2), ("XB", 3), ("XR", "h", 1, 1), ("TS",), ("XA", 1), ("XO", 0), ("W0", 3),
    ("XB", 1), ("OXY",), ("W0", 1), ("ST",), ("XA", 2), ("TB",), ("FILL",), ("XN", 3),
    ("XR", "n", 1, 1), ("XR", "n", 3, 1), ("XR", "h", 3, 2), ("WL", 3, 0), ("XO", 1),
    ("WL", 1, 3), ("XN", 1), ("XB2",), ("XR", "a", 1, 0), ("W0", 2), ("XR", "n", 3, 2),
    ("XN", 0), ("XO", 2), ("WL", 1, 1), ("WL", 1, 0), ("OR", "h", 3), ("OY",), ("XN", 2),
    ("XR", "a", 3, 1), ("WT", 3), ("WL", 3, 3), ("XR", "h", 1, 0), ("XR", "a", 1, 1),
    ("XR", "a", 3, 0), ("WL", 3, 1), ("OB", 1), ("XR", "n", 1, 0), ("OR", "h", 1),
    ("XR", "a", 1, 2), ("WL", 1, 2), ("XR", "n", 3, 0), ("WL", 3, 2), ("XR", "h", 3, 0),
    ("XR", "n", 1, 2), ("XR", "a", 3, 2), ("WT", 0), ("OB", 3), ("EARLY",), ("WT", 1),
    ("WT", 2), ("OA",), ("LATEX",), ("LATE",), ("heads",), ("ON", 1), ("level", 1), ("ON", 0),
    ("level", 2), ("OO",), ("OB2",), ("level", 3), ("level", 4), ("level", 5), ("level", 6),
    ("level", 7), ("maps",), ("join",), ("ON", 3), ("OR", "n", 3), ("OR", "a", 1),
    ("OR", "a", 3), ("pool",), ("ON", 2), ("OR", "n", 1), ("state",), ("finish",), ("GP",),
    ("GD",), ("WOALL",),
)


def dot(a, b, dims=((1,), (0,)), precision=None):
    return lax.dot_general(
        a, b, (dims, ((), ())), precision=precision, preferred_element_type=F32
    )


def iota(shape, dim):
    return lax.broadcasted_iota(jnp.int32, shape, dim)


def silu(a):
    return a * jax.nn.sigmoid(a)


def unit(a):
    return a * lax.rsqrt(jnp.sum(a * a, axis=-1, keepdims=True) + EPS)


def kernel(
    x_in, wp_in, wq_in, wk_in, wv_in, wg_in, op_in, od_in, pm_in,
    hld_in, dlb_in, wlb_in, gain_in, factor_in, offset_in, pscale_in, hng_in, dw_in, sw_in,
    out_ref,
    hld_v, dlb_v, wlb_v, gain_v, factor_v, offset_v, pscale_v, hng_v, rates_v, x_v, w_v, wo_v,
    xbuf, wbuf, wo, gain_f, pk_src, packb, pmb, xg, acc, ssq,
    w_stage, stc, stz_src, stz, pad, pool_src, delta_src, prev_src, ap, ad,
    rs2, rsp, rsm, rl, rin, o0, pmx, kw0_s, b0_s, keep_s, low_s, inv_s, up_s, down_s, state_s,
    in_rs, big_rs, near, ws_rs, x_rs, w_rs, wo_rs, pk_rs, pm_rs, st_rs, stz_rs, prev_rs, ap_rs, ad_rs, rs_rs,
    x_ss, xf_ss, w_ss, wf_ss, wo_ss, wof_ss, pk_ss, pm_ss, st_ss, stz_ss, prev_ss,
    ap_ss, ad_ss, apf_ss, adf_ss, rs_ss,
):
    sp, tp = lax.axis_index("sp"), lax.axis_index("tp")
    z, y = lax.div(sp, 4), lax.rem(sp, 4)
    x, c = lax.div(tp, 2), lax.rem(tp, 2)
    kh = lax.div(y, 2)
    yodd = lax.rem(y, 2)
    home = c == kh
    away = jnp.logical_not(home)

    def mod4(a):
        return lax.rem(a + 8, 4)

    def dev(zz, yy, xx, cc):
        return (4 * zz + yy, 2 * xx + cc)

    zp, zm, z2 = mod4(z + 1), mod4(z - 1), mod4(z + 2)
    yp, ym = mod4(y + 1), mod4(y - 1)
    xp, xm, x2 = mod4(x + 1), mod4(x - 1), mod4(x + 2)
    me_z, me_y, me_x = z, y, x
    partner = dev(z, y, x, 1 - c)

    ends = []

    def remote(src, dst, ssem, rsem, to, cond=None):
        def make():
            return pltpu.make_async_remote_copy(
                src_ref=src, dst_ref=dst, send_sem=ssem, recv_sem=rsem,
                device_id=to, device_id_type=MESH,
            )

        if cond is None:
            make().start()
            ends.append(lambda: make().wait_send())
        else:
            @pl.when(cond)
            def _():
                make().start()

            def end():
                @pl.when(cond)
                def _():
                    make().wait_send()

            ends.append(end)

    def arrived(ref, sem):
        pltpu.make_async_copy(ref, ref, sem).wait()

    loads = [
        (hld_in, hld_v), (dlb_in, dlb_v), (wlb_in, wlb_v), (factor_in, factor_v),
        (offset_in, offset_v), (pscale_in, pscale_v), (gain_in, gain_v), (hng_in, hng_v),
        (dw_in, rates_v.at[pl.ds(0, 16), :]), (sw_in, rates_v.at[pl.ds(16, 16), :]),
    ]
    big = [(x_in, x_v)]
    big += [(ref, w_v.at[n]) for n, ref in enumerate((wp_in, wq_in, wk_in, wv_in, wg_in))]
    big += [(ref, wo_v.at[n]) for n, ref in enumerate((op_in, od_in))]
    for i, (src, dst) in enumerate(big):
        pltpu.make_async_copy(src, dst, big_rs.at[i]).start()
    for i, (src, dst) in enumerate(loads):
        pltpu.make_async_copy(src, dst, in_rs.at[i]).start()

    barrier = pltpu.get_barrier_semaphore()
    peers = [partner]
    for d in (1, 3):
        for cc in (0, 1):
            peers.append(dev(mod4(z + d), y, x, cc))
            peers.append(dev(z, mod4(y + d), x, cc))
            peers.append(dev(z, y, mod4(x + d), cc))
    for to in peers:
        pl.semaphore_signal(barrier, inc=1, device_id=to, device_id_type=MESH)
    pl.semaphore_wait(barrier, len(peers))
    for to in (dev(zp, y, x, c), dev(zm, y, x, c), dev(z, yp, x, c), dev(z, ym, x, c)):
        pl.semaphore_signal(near, inc=1, device_id=to, device_id_type=MESH)
    for i, (src, dst) in enumerate(big):
        pltpu.make_async_copy(src, dst, big_rs.at[i]).wait()

    def xslot(yy, xx, u, quarter=None):
        start, size = PARTS[u]
        if quarter is not None:
            start, size = start + size // 2 * quarter, size // 2
        return xbuf.at[2 * xx + u // 2, pl.ds(256 * lax.rem(yy, 2) + start, size), :]

    def xsem(yy, xx, u):
        return x_rs.at[16 * lax.rem(yy, 2) + 4 * xx + u]

    def wslot(zz, yy, r):
        return wbuf.at[2 * (4 * zz + yy) + r, :, pl.ds(0, 640)]

    def wsem(zz, yy, r):
        return w_rs.at[2 * (4 * zz + yy) + r]

    def woslot(zz, yy, cc, half=None):
        block = wo.at[zz, 2 * lax.rem(yy, 2) + cc]
        return block if half is None else block.at[pl.ds(256 * half, 256), :]

    def wosem(zz, yy, cc):
        return wo_rs.at[4 * zz + 2 * lax.rem(yy, 2) + cc]

    def own_x(u):
        start, size = PARTS[u]
        return x_v.at[pl.ds(start, size), :], xslot(y, x, u), xsem(y, x, u)

    def own_x_along_y(u):
        src, dst, sem = own_x(u)
        for i, yy in enumerate((yp, ym)):
            remote(src, dst, x_ss.at[12 + 2 * u + i], sem, dev(z, yy, x, kh), c == u // 2)

    def both(p, q):
        return jnp.logical_and(p, q)

    wo_own = wo.at[z, 2 * yodd + c]
    own_sem = wo_rs.at[4 * z + 2 * yodd + c]

    def own_wo(tos, at):
        for half, ref in enumerate((op_in, od_in)):
            part = wo_own.at[pl.ds(256 * half, 256), :]
            for i, to in enumerate(tos):
                remote(wo_v.at[half], part, wo_ss.at[at + 2 * half + i], own_sem, to)

    yn = 2 * c + 1 - yodd
    yo = 2 * c + yodd
    from_below = mod4(yn + 1) == y
    relay_half = jnp.where(from_below, 0, 1)
    y_next = jnp.where(from_below, yp, ym)
    xf_n, wf_n, wof_n = iter(range(64)), iter(range(64)), iter(range(64))
    x_ring = (dev(z, y, xp, c), dev(z, y, xm, c))
    y_ring = (dev(z, yp, x, c), dev(z, ym, x, c))
    z_ring = (dev(zp, y, x, c), dev(zm, y, x, c))
    y_relay = (relay_half, dev(z, y_next, x, c))
    x_relay = {3: (0, x_ring[0]), 1: (1, x_ring[1])}
    z_relay = {3: (0, z_ring[0]), 1: (1, z_ring[1])}
    x_at, z_at = (x, xp, x2, xm), (z, zp, z2, zm)
    cases = {"n": (yn, None), "h": (yo, home), "a": (yo, away)}
    seen = set()

    def take(key, slot, sem, cond=None):
        if key in seen:
            return
        seen.add(key)
        if cond is None:
            arrived(slot, sem)
        else:
            @pl.when(cond)
            def _():
                arrived(slot, sem)

    def x_take(case, d, u):
        yy, cond = cases[case]
        take(("x", case, d, u), xslot(yy, x_at[d], u), xsem(yy, x_at[d], u), cond)

    def x_pass(case, d, u, tos, relay=None):
        x_take(case, d, u)
        yy, cond = cases[case]
        slot, sem = xslot(yy, x_at[d], u), xsem(yy, x_at[d], u)
        for to in tos:
            remote(slot, slot, xf_ss.at[next(xf_n)], sem, to, cond)
        if relay is not None:
            half, to = relay
            part = xslot(yy, x_at[d], u, half)
            remote(part, part, xf_ss.at[next(xf_n)], sem, to, cond)

    def o_take(case, d, cc):
        yy, cond = cases[case]
        take(("o", case, d, cc), woslot(z_at[d], yy, cc), wosem(z_at[d], yy, cc), cond)

    def o_pass(case, d, cc, tos, relay=None):
        o_take(case, d, cc)
        yy, cond = cases[case]
        slot, sem = woslot(z_at[d], yy, cc), wosem(z_at[d], yy, cc)
        for to in tos:
            remote(slot, slot, wof_ss.at[next(wof_n)], sem, to, cond)
        if relay is not None:
            half, to = relay
            part = woslot(z_at[d], yy, cc, half)
            remote(part, part, wof_ss.at[next(wof_n)], sem, to, cond)

    def w_take(d, e, r, tag):
        yy = mod4(me_y + e)
        take((tag, d, e), wslot(z_at[d], yy, r), wsem(z_at[d], yy, r))

    def w_pass(d, e, tos):
        w_take(d, e, c, "w")
        yy = mod4(me_y + e)
        slot, sem = wslot(z_at[d], yy, c), wsem(z_at[d], yy, c)
        for to in (*tos, partner):
            remote(slot, slot, wf_ss.at[next(wf_n)], sem, to)

    def fill(i, carry):
        rows = pl.ds(pl.multiple_of(512 * i, 512), 512)
        both_cols = dot(rates_v[:, rows], pick, ((0,), (0,))).astype(BF16)
        wbuf[pl.ds(4 * i, 4), :, 640:768] = both_cols.reshape(4, 128, 128)
        return carry

    head = 4 * x + y
    row32, col32 = iota((32, 128), 0), iota((32, 128), 1)
    pick = jnp.logical_or(
        jnp.logical_and(row32 == head, col32 == 0),
        jnp.logical_and(row32 == head + 16, col32 == 1),
    ).astype(BF16)

    def project(i):
        total = acc[...]
        for k in (0, 1):
            gains = [gain_f[pl.ds(8 * i + 4 * k + q, 1), :] for q in range(4)]
            gain = jnp.concatenate(gains, axis=1)
            for b in range(4):
                rows = slice(128 * b, 128 * b + 128)
                v = xbuf[2 * i + k, rows, :].astype(F32)
                sq = v * v
                ssq[rows, :] += (
                    (sq[:, 0:128] + sq[:, 128:256]) + (sq[:, 256:384] + sq[:, 384:512])
                )
                xg[k, rows, :] = (v * gain).astype(BF16)
            total = total + dot(xg[k], wbuf[pl.ds(8 * i + 4 * k, 4)].reshape(512, 768))
        acc[...] = total

    ii, jj = iota((256, 256), 0), iota((256, 256), 1)
    diff = jnp.bitwise_xor(ii, jj)
    lower = ii > jj
    causal = ii >= jj
    upto = (ii <= jj).astype(F32)
    eye = (ii == jj).astype(F32)

    def row_scale(b):
        total = jnp.sum(ssq[256 * b : 256 * b + 256, :], axis=-1, keepdims=True)
        return lax.rsqrt(total * (1.0 / 4096.0) + EPS)

    prev_to = dev(jnp.where(c == 0, z, zp), y, x, 1 - c)
    last = jnp.logical_and(z == 3, c == 1)
    first = jnp.logical_and(z == 0, c == 0)
    prev_dst = ap.at[pl.ds(256, 16), pl.ds(0, 128)]
    heads = []
    maps = []

    def spread_out(src, dst, rsem, ssem):
        cols = pl.ds(128 * y, 128)

        @pl.when(home)
        def _():
            dst[0:256, cols] = src[pl.ds(256 * yodd, 256), :]

        for j in (0, 1):
            to_y = 2 * c + j
            here = to_y == y
            rows = pl.ds(256 * j, 256)
            remote(
                src.at[rows, :], dst.at[pl.ds(0, 256), cols], ssem.at[3 * j],
                rsem.at[y], partner, here,
            )
            for r in (0, 1):
                remote(
                    src.at[pl.ds(256 * j + 128 * r, 128), :],
                    dst.at[pl.ds(128 * r, 128), cols],
                    ssem.at[3 * j + 1 + r], rsem.at[y], dev(z, to_y, x, r),
                    jnp.logical_not(here),
                )

    def t_x():
        for half in (1, 0):
            for cc in (0, 1):
                u = 2 * cc + half
                src, dst, sem = own_x(u)
                for i, xx in enumerate((xp, xm)):
                    remote(src, dst, x_ss.at[3 * u + i], sem, dev(z, y, xx, kh), c == cc)
                mine = c == cc
                remote(src, dst, x_ss.at[3 * u + 2], sem, partner, both(mine, away))

                @pl.when(both(mine, home))
                def _(u=u, dst=dst, sem=sem):
                    start, size = PARTS[u]
                    pltpu.make_async_copy(x_in.at[pl.ds(start, size), :], dst, sem).start()

    def t_y():
        for u in (0, 1, 2):
            own_x_along_y(u)

    def t_s():
        for j in (0, 1):
            same = yodd == j
            for r in (0, 1):
                far = dev(z, yp if r == 0 else ym, x, r)
                for n, ref in enumerate((wp_in, wq_in, wk_in, wv_in, wg_in)):
                    src = w_v.at[n, pl.ds(128 * r, 128), pl.ds(128 * j, 128)]
                    dst = w_stage.at[:, pl.ds(128 * n, 128)]
                    remote(src, dst, w_ss.at[10 * j + 5 * r + n], ws_rs.at[0], far, both(away, same))

    def t_w():
        for j in (0, 1):
            same = yodd == j
            head_y = 2 * c + j
            for r in (0, 1):
                here = both(both(home, same), c == r)
                direct = jnp.logical_not(jnp.logical_or(here, both(away, same)))
                for n, ref in enumerate((wp_in, wq_in, wk_in, wv_in, wg_in)):
                    src = ref.at[pl.ds(128 * r, 128), pl.ds(128 * j, 128)]
                    dst = wbuf.at[2 * sp + r, :, pl.ds(128 * n, 128)]
                    here_v = w_v.at[n, pl.ds(128 * r, 128), pl.ds(128 * j, 128)]
                    remote(
                        here_v, dst, w_ss.at[20 + 10 * j + 5 * r + n], wsem(z, y, r),
                        dev(z, head_y, x, r), direct,
                    )

                    @pl.when(here)
                    def _(src=src, dst=dst, r=r):
                        pltpu.make_async_copy(src, dst, wsem(z, y, r)).start()

        for half, ref in enumerate((op_in, od_in)):
            part = wo_own.at[pl.ds(256 * half, 256), :]
            remote(wo_v.at[half], part, wo_ss.at[8 + half], own_sem, partner, away)

            @pl.when(home)
            def _(ref=ref, part=part):
                pltpu.make_async_copy(ref, part, own_sem).start()

    def t_b():
        for i, (src, dst) in enumerate(loads):
            pltpu.make_async_copy(src, dst, in_rs.at[i]).wait()
        pk_src[0:2, :] = factor_v[...]
        pk_src[2:4, :] = offset_v[...]
        for j in (0, 1):
            for at, ref in ((4, hld_v), (6, dlb_v), (8, wlb_v)):
                pk_src[at + j : at + j + 1, :] = jnp.broadcast_to(ref[0:1, j : j + 1], (1, 256))
        pk_src[10:11, :] = pscale_v[...]
        for j in (0, 1):
            head_y = 2 * c + j
            self_here = jnp.logical_and(head_y == y, home)
            remote(
                pk_src, packb.at[yodd], pk_ss.at[j], pk_rs.at[yodd], dev(z, head_y, x, kh),
                jnp.logical_not(self_here),
            )

            @pl.when(self_here)
            def _():
                packb[yodd] = pk_src[...]

        remote(pm_in.at[yodd], pmb, pm_ss.at[0], pm_rs.at[0], partner, home)

        @pl.when(home)
        def _():
            pltpu.make_async_copy(pm_in.at[yodd], pmb, pm_rs.at[0]).start()

    def stage():
        arrived(w_stage, ws_rs.at[0])
        stage_from = jnp.where(c == 0, ym, yp)
        stage_to = jnp.where(c == 0, yp, ym)
        stage_dst = wbuf.at[2 * (4 * z + stage_from) + c, :, pl.ds(0, 640)]
        remote(w_stage, stage_dst, w_ss.at[40], wsem(z, stage_from, c), dev(z, stage_to, x, c))

    def start_rates():
        lax.fori_loop(0, 8, fill, 0)
        gain_f[...] = gain_v[...].astype(F32)
        ssq[...] = jnp.zeros_like(ssq)
        acc[...] = jnp.zeros_like(acc)

    gap = mod4(x - z)

    def depth(parts, ds):
        for d in ds:
            for case in "nha":
                for u in range(4):
                    x_take(case, d, u)
            for e in (0, 1, 2, 3):
                w_take(d, e, c, "w")
                w_take(d, e, 1 - c, "p")
        for i in parts:
            project(i)

    def early():
        first_part = jnp.where(gap == 2, xp, x)
        depth((first_part, jnp.where(gap == 2, xm, jnp.where(gap == 0, xp, z))), (0, 1, 3))

    def late_x():
        for case in "nha":
            for u in range(4):
                x_take(case, 2, u)
        project(jnp.where(gap == 0, xm, jnp.where(gap == 2, z, x2)))

    def late():
        depth((jnp.where(gap == 0, x2, jnp.where(gap == 2, x, z2)),), (2,))

    def delta_heads():
        for b in (0, 1):
            @pl.when(jnp.logical_or(away, yodd != b))
            def _(b=b):
                arrived(packb.at[b], pk_rs.at[b])
        arrived(pmb, pm_rs.at[0])

        scale = [row_scale(0), row_scale(1)]

        for b in (0, 1):
            pad[16 + 256 * b : 272 + 256 * b, :] = acc[256 * b : 256 * b + 256, 0:128] * scale[b]
        prev_src[...] = pad[512:528, :].astype(BF16)
        remote(prev_src, prev_dst, prev_ss.at[0], prev_rs.at[0], prev_to, jnp.logical_not(last))

        for b in (0, 1):
            rows = slice(256 * b, 256 * b + 256)
            s = scale[b]
            q = unit(silu(acc[rows, 128:256] * s)) * HD ** (-0.5)
            k = unit(silu(acc[rows, 256:384] * s))
            v = silu(acc[rows, 384:512] * s)
            rate = acc[rows, 640:768] * s
            table = packb[b]
            of = lambda r: jnp.where(yodd == 0, table[r : r + 1, :], table[r + 1 : r + 2, :])
            factor, offset, hld, dlb, wlb = (of(r) for r in (0, 2, 4, 6, 8))
            pre = rate.T[0:1, :] + dlb
            soft = jnp.maximum(pre, 0.0) + jnp.log1p(jnp.exp(-jnp.abs(pre)))
            log_decay = -jnp.exp(hld) * soft * factor + offset
            run_row = dot(jnp.broadcast_to(log_decay, (8, 256)), upto, precision=HIGHEST)[0:1, :]
            run = jnp.broadcast_to(run_row, (128, 256)).T
            beta = jax.nn.sigmoid(rate[:, 1:2] + wlb[:, 0:1])
            spread = jnp.concatenate([run, run], axis=1) - run_row
            decay = jnp.where(causal, jnp.exp(jnp.where(causal, spread, 0.0)), 0.0)
            k16, q16 = k.astype(BF16), q.astype(BF16)
            low = jnp.where(lower, dot(k16, k16, ((1,), (1,))) * (decay * beta), 0.0)
            scores = (dot(q16, k16, ((1,), (1,))) * decay).astype(BF16)
            inverse = eye - jnp.where(diff == 1, low, 0.0)
            grown = jnp.exp(run)
            kb = k * beta
            low_s[b] = low
            inv_s[b] = inverse
            heads.append(dict(q=q, k=k, v=v, scores=scores, run=run, grown=grown, kb=kb, beta=beta))

    def level_step(level):
        mask = jnp.right_shift(diff, level) == 1
        mids = []
        for b in (0, 1):
            off = jnp.where(mask, low_s[b], 0.0).astype(BF16)
            mids.append(dot(off, inv_s[b].astype(BF16)).astype(BF16))
        for b, mid in enumerate(mids):
            inv_s[b] = inv_s[b] - dot(inv_s[b].astype(BF16), mid)

    def delta_maps():
        for b, h in enumerate(heads):
            rows = slice(256 * b, 256 * b + 256)
            rhs = jnp.concatenate([h["v"] * h["beta"], h["kb"] * h["grown"]], axis=1)
            uw = rhs + dot((inv_s[b] - eye).astype(BF16), rhs.astype(BF16))
            uw16 = uw.astype(BF16)
            both = dot(h["scores"], uw16)
            o0[rows, :] = both[:, 0:128]
            pmx[rows, :] = (h["q"] * h["grown"] - both[:, 128:256]).astype(BF16)
            last_run = h["run"][255:256, :]
            kd = (h["k"] * jnp.exp(last_run - h["run"])).astype(BF16)
            ku = dot(kd, uw16, ((0,), (0,)))
            keep = jnp.exp(last_run)
            maps.append((keep, ku[:, 128:256].astype(BF16), ku[:, 0:128]))

        eye128 = (iota((128, 128), 0) == iota((128, 128), 1)).astype(F32)
        keep0, kw0, b0 = maps[0]
        keep1, kw1, b1 = maps[1]
        m0 = eye128 * keep0 - kw0.astype(F32)
        kw0_s[...] = kw0
        b0_s[...] = b0
        keep_s[0:1, :] = keep0
        first_map = jnp.concatenate([m0, b0], axis=1)
        keep1w = jnp.concatenate([keep1, keep1], axis=1)
        core_map = keep1w * first_map - dot(kw1, first_map.astype(BF16))
        core_map = core_map + jnp.concatenate([jnp.zeros_like(b1), b1], axis=1)
        stc[c] = core_map.astype(BF16)
        remote(stc.at[c], stc.at[c], st_ss.at[0], st_rs.at[c], partner)

    def join_maps():
        arrived(stc.at[1 - c], st_rs.at[1 - c])
        one = stc[1]
        chip_map = dot(one[:, 0:128], stc[0])
        chip_map = chip_map + jnp.concatenate([jnp.zeros((128, 128), F32), one[:, 128:256].astype(F32)], axis=1)
        stz_src[...] = chip_map.astype(BF16)
        pl.semaphore_wait(near, 4)
        for d in (2, 1, 3):
            remote(
                stz_src, stz.at[z], stz_ss.at[d - 1], stz_rs.at[z],
                dev(mod4(z + d), y, x, c), z + d <= 3,
            )

    def pool_part():
        @pl.when(first)
        def _():
            pad[0:16, :] = jnp.zeros((16, 128), F32)

        @pl.when(jnp.logical_not(first))
        def _():
            arrived(prev_dst, prev_rs.at[0])
            pad[0:16, :] = ap[256:272, 0:128].astype(F32)

        window = jnp.left_shift(2, y)
        base = 512 * (2 * z + c)
        for b in (0, 1):
            at = 256 * b
            sums = pad[16 + at : 272 + at, :]
            here = sums
            for lag in range(1, 16):
                part = pad[16 + at - lag : 272 + at - lag, :]
                sums = sums + part * jnp.where(lag < window, 1.0, 0.0)
            counts = jnp.minimum(base + at + iota((256, 128), 0) + 1, window).astype(F32)
            pooled = (sums / counts - here).astype(BF16)
            row = packb[b]
            pscale = jnp.where(yodd == 0, row[10:11, 0:128], row[10:11, 128:256])
            pool_src[at : at + 256, :] = (dot(pooled, pmb[...]) * pscale).astype(BF16)

        spread_out(pool_src, ap, ap_rs, ap_ss)

    def state_in():
        state_s[...] = jnp.zeros((128, 128), F32)

        def absorb(part):
            moved = dot(part[:, 0:128], state_s[...].astype(BF16))
            state_s[...] = moved + part[:, 128:256].astype(F32)

        for i in (0, 1, 2):
            @pl.when(i < z)
            def _(i=i):
                arrived(stz.at[i], stz_rs.at[i])
                absorb(stz[i])

        @pl.when(c == 1)
        def _():
            absorb(stc[0])

    def finish():
        hng = hng_v[...]
        for b in (0, 1):
            rows = slice(256 * b, 256 * b + 256)
            s16 = state_s[...].astype(BF16)
            o = o0[rows, :] + dot(pmx[rows, :], s16)
            gate = silu(acc[rows, 512:640] * row_scale(b))
            norm = lax.rsqrt(jnp.mean(o * o, axis=-1, keepdims=True) + EPS)
            delta_src[rows, :] = (o * norm * hng * gate).astype(BF16)
            if b == 0:
                state_s[...] = keep_s[0:1, :] * state_s[...] - dot(kw0_s[...], s16) + b0_s[...]

        spread_out(delta_src, ad, ad_rs, ad_ss)

    def pass_on(dst, rsem, fsem):
        for i, d in enumerate((1, 3, 2)):
            yy = mod4(me_y + d)
            part = dst.at[pl.ds(128 * c, 128), pl.ds(128 * yy, 128)]
            arrived(part, rsem.at[yy])
            remote(part, part, fsem.at[i], rsem.at[4 + yy], partner)

    def from_partner(dst, rsem):
        for d in (1, 3, 2):
            yy = mod4(me_y + d)
            part = dst.at[pl.ds(128 * (1 - c), 128), pl.ds(128 * yy, 128)]
            arrived(part, rsem.at[4 + yy])

        @pl.when(away)
        def _():
            arrived(dst.at[pl.ds(0, 256), pl.ds(128 * me_y, 128)], rsem.at[me_y])

    def rest_of_output_weights():
        for d in range(4):
            for case in "nha":
                for cc in (0, 1):
                    o_take(case, d, cc)
        from_partner(ap, ap_rs)
        from_partner(ad, ad_rs)

    ops = dict(
        TX=t_x, GP=lambda: pass_on(ap, ap_rs, apf_ss),
        GD=lambda: pass_on(ad, ad_rs, adf_ss), TY=t_y, TS=t_s, TW=t_w, TB=t_b, ST=stage, FILL=start_rates, EARLY=early,
        LATEX=late_x, LATE=late, heads=delta_heads, level=level_step, maps=delta_maps, join=join_maps,
        pool=pool_part, state=state_in, finish=finish, WOALL=rest_of_output_weights,
        W0=lambda e: w_pass(0, e, z_ring),
        WL=lambda d, e: w_pass(d, e, (z_relay[d][1],) if (d == 3) == (e in (0, 2)) else ()),
        WT=lambda e: w_pass(2, e, ()),
        XA=lambda u: x_pass("n", 0, u, x_ring, y_relay),
        XO=lambda u: x_pass("a", 0, u, x_ring),
        XB=lambda d: x_pass("h", d, 3, y_ring, x_relay[d]),
        XB2=lambda: x_pass("h", 2, 3, y_ring),
        XN=lambda d: x_pass("n", d, 3, (), y_relay),
        XR=lambda case, d, u: x_pass(case, d, u, (), x_relay[d]),
        OXY=lambda: own_x_along_y(3),
        OY=lambda: own_wo((dev(z, yp, x, kh), dev(z, ym, x, kh)), 4),
        OZ=lambda: own_wo((dev(zp, y, x, kh), dev(zm, y, x, kh)), 0),
        OA=lambda: o_pass("n", 0, 1, z_ring, y_relay),
        OO=lambda: o_pass("a", 0, 1, z_ring),
        OB=lambda d: o_pass("h", d, 0, y_ring, z_relay[d]),
        OB2=lambda: o_pass("h", 2, 0, y_ring),
        ON=lambda d: o_pass("n", d, 0, (), y_relay),
        OR=lambda case, d: o_pass(case, d, 1, (), z_relay[d]),
    )
    for name, *args in SCHEDULE:
        ops[name](*args)

    def piece(zz):
        halves = []
        for j in (0, 1):
            part = None
            for cc in (0, 1):
                cols = slice(256 * cc, 256 * cc + 256)
                term = dot(ap[0:256, cols], wo[zz, 2 * j + cc, 0:256, :])
                term = term + dot(ad[0:256, cols], wo[zz, 2 * j + cc, 256:512, :])
                part = term if part is None else part + term
            halves.append(part)
        return jnp.concatenate(halves, axis=1)

    top, bottom = pl.ds(0, 128), pl.ds(128, 128)
    to_p, to_m = dev(z, y, xp, c), dev(z, y, xm, c)
    rs2[...] = piece(x2).astype(BF16)
    remote(rs2.at[top, :], rl.at[0], rs_ss.at[0], rs_rs.at[0], to_p)
    remote(rs2.at[bottom, :], rl.at[1], rs_ss.at[1], rs_rs.at[1], to_m)
    up_s[...] = piece(xp)
    rsp[128:256, :] = up_s[128:256, :].astype(BF16)
    remote(rsp.at[bottom, :], rin.at[0, bottom, :], rs_ss.at[2], rs_rs.at[2], to_p)
    down_s[...] = piece(xm)
    rsm[0:128, :] = down_s[0:128, :].astype(BF16)
    remote(rsm.at[top, :], rin.at[1, top, :], rs_ss.at[3], rs_rs.at[3], to_m)
    arrived(rl.at[0], rs_rs.at[0])
    rsp[0:128, :] = (up_s[0:128, :] + rl[0].astype(F32)).astype(BF16)
    remote(rsp.at[top, :], rin.at[0, top, :], rs_ss.at[4], rs_rs.at[4], to_p)
    arrived(rl.at[1], rs_rs.at[1])
    rsm[128:256, :] = (down_s[128:256, :] + rl[1].astype(F32)).astype(BF16)
    remote(rsm.at[bottom, :], rin.at[1, bottom, :], rs_ss.at[5], rs_rs.at[5], to_m)
    mine = piece(x)
    arrived(rin.at[0, bottom, :], rs_rs.at[2])
    arrived(rin.at[1, top, :], rs_rs.at[3])
    arrived(rin.at[0, top, :], rs_rs.at[4])
    arrived(rin.at[1, bottom, :], rs_rs.at[5])
    out_ref[...] = (mine + rin[0].astype(F32) + rin[1].astype(F32)).astype(BF16)

    for end in ends:
        end()


def per_device(
    inputs, input_norm_gain, pooling_input_weight, query_weight, key_weight,
    value_weight, gate_weight, decay_weight, strength_weight, pooling_group_map,
    pooling_scale, head_log_decay, decay_logit_bias, write_logit_bias,
    decay_position_factor, decay_position_offset, head_norm_gain,
    pooling_output_weight, delta_output_weight,
):
    dma = pltpu.SemaphoreType.DMA
    vmem = pltpu.VMEM
    hbm = pl.BlockSpec(memory_space=pl.ANY)
    local = pl.BlockSpec(memory_space=pltpu.VMEM)
    return pl.pallas_call(
        kernel,
        out_shape=pltpu.VMEM((256, 512), BF16),
        in_specs=[hbm] * 19,
        out_specs=local,
        scratch_shapes=[
            vmem((1, 2), F32),
            vmem((1, 2), F32),
            vmem((1, 2), F32),
            vmem((32, 128), BF16),
            vmem((2, 256), F32),
            vmem((2, 256), F32),
            vmem((1, 256), F32),
            vmem((1, 128), F32),
            vmem((32, 4096), BF16),
            vmem((256, 512), BF16),
            vmem((5, 256, 256), BF16),
            vmem((2, 256, 256), BF16),
            vmem((8, 512, 512), BF16),
            vmem((32, 128, 768), BF16),
            vmem((4, 4, 512, 256), BF16),
            vmem((32, 128), F32),
            vmem((16, 256), F32),
            vmem((2, 16, 256), F32),
            vmem((128, 128), BF16),
            vmem((2, 512, 512), BF16),
            vmem((512, 768), F32),
            vmem((512, 128), F32),
            vmem((128, 640), BF16),
            vmem((2, 128, 256), BF16),
            vmem((128, 256), BF16),
            vmem((4, 128, 256), BF16),
            vmem((528, 128), F32),
            vmem((512, 128), BF16),
            vmem((512, 128), BF16),
            vmem((16, 128), BF16),
            vmem((272, 512), BF16),
            vmem((256, 512), BF16),
            vmem((256, 512), BF16),
            vmem((256, 512), BF16),
            vmem((256, 512), BF16),
            vmem((2, 128, 512), BF16),
            vmem((2, 256, 512), BF16),
            vmem((512, 128), F32),
            vmem((512, 128), BF16),
            vmem((128, 128), BF16),
            vmem((128, 128), F32),
            vmem((8, 128), F32),
            vmem((2, 256, 256), F32),
            vmem((2, 256, 256), F32),
            vmem((256, 512), F32),
            vmem((256, 512), F32),
            vmem((128, 128), F32),
            dma((10,)), dma((8,)), pltpu.SemaphoreType.REGULAR, dma((1,)), dma((32,)), dma((32,)), dma((16,)), dma((2,)), dma((1,)), dma((2,)),
            dma((4,)), dma((1,)), dma((8,)), dma((8,)), dma((6,)),
            dma((20,)), dma((48,)), dma((41,)), dma((32,)), dma((10,)), dma((32,)),
            dma((2,)), dma((1,)), dma((1,)), dma((3,)), dma((1,)),
            dma((6,)), dma((6,)), dma((3,)), dma((3,)), dma((6,)),
        ],
        compiler_params=pltpu.CompilerParams(
            collective_id=0, has_side_effects=True, vmem_limit_bytes=60 * 1024 * 1024
        ),
    )(
        inputs, pooling_input_weight, query_weight, key_weight, value_weight,
        gate_weight, pooling_output_weight, delta_output_weight, pooling_group_map,
        head_log_decay[None], decay_logit_bias[None], write_logit_bias[None],
        input_norm_gain.reshape(32, 128), decay_position_factor.T, decay_position_offset.T,
        pooling_scale[None], head_norm_gain[None], decay_weight.T, strength_weight.T,
    )


def solution(mesh):
    rows, heads = P("sp", "tp"), P("tp")
    in_specs = (
        rows, P(), rows, rows, rows, rows, rows, P(), P(), P("tp", None, None),
        heads, heads, heads, heads, rows, rows, P(), P("tp", "sp"), P("tp", "sp"),
    )
    return jax.shard_map(
        per_device, mesh=mesh, in_specs=in_specs, out_specs=rows, check_vma=False
    )
```

```python
import functools

import jax
import jax.numpy as jnp
from jax import lax
from jax.experimental import pallas as pl
from jax.experimental.pallas import tpu as pltpu
from jax.sharding import PartitionSpec as P

MESH = pl.DeviceIdType.MESH
F32 = jnp.float32
BF16 = jnp.bfloat16
HD = 128
EPS = 1e-06
PARTS = ((0, 128), (128, 128), (0, 128), (128, 128))
HIGHEST = lax.Precision.HIGHEST


SCHEDULE = (
    ("TX",), ("TY",), ("TW",), ("OZ",), ("XR", "h", 3, 1), ("XA", 0), ("W0", 0),
    ("XR", "h", 1, 2), ("XB", 3), ("XR", "h", 1, 1), ("TS",), ("XA", 1), ("XO", 0), ("W0", 3),
    ("XB", 1), ("OXY",), ("W0", 1), ("ST",), ("XA", 2), ("TB",), ("FILL",), ("XN", 3),
    ("XR", "n", 1, 1), ("XR", "n", 3, 1), ("XR", "h", 3, 2), ("WL", 3, 0), ("XO", 1),
    ("WL", 1, 3), ("XN", 1), ("XB2",), ("XR", "a", 1, 0), ("W0", 2), ("XR", "n", 3, 2),
    ("XN", 0), ("XO", 2), ("WL", 1, 1), ("WL", 1, 0), ("OR", "h", 3), ("OY",), ("XN", 2),
    ("XR", "a", 3, 1), ("WT", 3), ("WL", 3, 3), ("XR", "h", 1, 0), ("XR", "a", 1, 1),
    ("XR", "a", 3, 0), ("WL", 3, 1), ("OB", 1), ("XR", "n", 1, 0), ("OR", "h", 1),
    ("XR", "a", 1, 2), ("WL", 1, 2), ("XR", "n", 3, 0), ("WL", 3, 2), ("XR", "h", 3, 0),
    ("XR", "n", 1, 2), ("XR", "a", 3, 2), ("WT", 0), ("OB", 3), ("EARLY",), ("WT", 1),
    ("WT", 2), ("OA",), ("LATEX",), ("LATE",), ("heads",), ("ON", 1), ("level", 1), ("ON", 0),
    ("level", 2), ("OO",), ("OB2",), ("level", 3), ("level", 4), ("level", 5), ("level", 6),
    ("level", 7), ("maps",), ("pool",), ("join",), ("ON", 3), ("OR", "n", 3), ("OR", "a", 1),
    ("OR", "a", 3), ("ON", 2), ("OR", "n", 1), ("state",), ("finish",), ("GP",), ("GD",),
    ("WOALL",),
)


def dot(a, b, dims=((1,), (0,)), precision=None):
    return lax.dot_general(
        a, b, (dims, ((), ())), precision=precision, preferred_element_type=F32
    )


def iota(shape, dim):
    return lax.broadcasted_iota(jnp.int32, shape, dim)


def silu(a):
    return a * jax.nn.sigmoid(a)


def unit(a):
    return a * lax.rsqrt(jnp.sum(a * a, axis=-1, keepdims=True) + EPS)


def kernel(
    x_in, wp_in, wq_in, wk_in, wv_in, wg_in, op_in, od_in, pm_in,
    hld_in, dlb_in, wlb_in, gain_in, factor_in, offset_in, pscale_in, hng_in, dw_in, sw_in,
    out_ref,
    hld_v, dlb_v, wlb_v, gain_v, factor_v, offset_v, pscale_v, hng_v, rates_v, x_v, w_v, wo_v,
    xbuf, wbuf, wo, gain_f, pk_src, packb, pmb, xg, acc, ssq,
    w_stage, stc, stz_src, stz, pad, pool_src, delta_src, prev_src, ap, ad,
    rs2, rsp, rsm, rl, rin, o0, pmx, kw0_s, b0_s, keep_s, low_s, inv_s, up_s, down_s, state_s,
    in_rs, big_rs, near, ws_rs, x_rs, w_rs, wo_rs, pk_rs, pm_rs, st_rs, stz_rs, prev_rs, ap_rs, ad_rs, rs_rs,
    x_ss, xf_ss, w_ss, wf_ss, wo_ss, wof_ss, pk_ss, pm_ss, st_ss, stz_ss, prev_ss,
    ap_ss, ad_ss, apf_ss, adf_ss, rs_ss,
):
    sp, tp = lax.axis_index("sp"), lax.axis_index("tp")
    z, y = lax.div(sp, 4), lax.rem(sp, 4)
    x, c = lax.div(tp, 2), lax.rem(tp, 2)
    kh = lax.div(y, 2)
    yodd = lax.rem(y, 2)
    home = c == kh
    away = jnp.logical_not(home)

    def mod4(a):
        return lax.rem(a + 8, 4)

    def dev(zz, yy, xx, cc):
        return (4 * zz + yy, 2 * xx + cc)

    zp, zm, z2 = mod4(z + 1), mod4(z - 1), mod4(z + 2)
    yp, ym = mod4(y + 1), mod4(y - 1)
    xp, xm, x2 = mod4(x + 1), mod4(x - 1), mod4(x + 2)
    me_z, me_y, me_x = z, y, x
    partner = dev(z, y, x, 1 - c)

    ends = []

    def remote(src, dst, ssem, rsem, to, cond=None):
        def make():
            return pltpu.make_async_remote_copy(
                src_ref=src, dst_ref=dst, send_sem=ssem, recv_sem=rsem,
                device_id=to, device_id_type=MESH,
            )

        if cond is None:
            make().start()
            ends.append(lambda: make().wait_send())
        else:
            @pl.when(cond)
            def _():
                make().start()

            def end():
                @pl.when(cond)
                def _():
                    make().wait_send()

            ends.append(end)

    def arrived(ref, sem):
        pltpu.make_async_copy(ref, ref, sem).wait()

    loads = [
        (hld_in, hld_v), (dlb_in, dlb_v), (wlb_in, wlb_v), (factor_in, factor_v),
        (offset_in, offset_v), (pscale_in, pscale_v), (gain_in, gain_v), (hng_in, hng_v),
        (dw_in, rates_v.at[pl.ds(0, 16), :]), (sw_in, rates_v.at[pl.ds(16, 16), :]),
    ]
    big = [(x_in, x_v)]
    big += [(ref, w_v.at[n]) for n, ref in enumerate((wp_in, wq_in, wk_in, wv_in, wg_in))]
    big += [(ref, wo_v.at[n]) for n, ref in enumerate((op_in, od_in))]
    for i, (src, dst) in enumerate(big):
        pltpu.make_async_copy(src, dst, big_rs.at[i]).start()
    for i, (src, dst) in enumerate(loads):
        pltpu.make_async_copy(src, dst, in_rs.at[i]).start()

    barrier = pltpu.get_barrier_semaphore()
    peers = [partner]
    for d in (1, 3):
        for cc in (0, 1):
            peers.append(dev(mod4(z + d), y, x, cc))
            peers.append(dev(z, mod4(y + d), x, cc))
            peers.append(dev(z, y, mod4(x + d), cc))
    for to in peers:
        pl.semaphore_signal(barrier, inc=1, device_id=to, device_id_type=MESH)
    pl.semaphore_wait(barrier, len(peers))
    for to in (dev(zp, y, x, c), dev(zm, y, x, c), dev(z, yp, x, c), dev(z, ym, x, c)):
        pl.semaphore_signal(near, inc=1, device_id=to, device_id_type=MESH)
    for i, (src, dst) in enumerate(big):
        pltpu.make_async_copy(src, dst, big_rs.at[i]).wait()

    def xslot(yy, xx, u, quarter=None):
        start, size = PARTS[u]
        if quarter is not None:
            start, size = start + size // 2 * quarter, size // 2
        return xbuf.at[2 * xx + u // 2, pl.ds(256 * lax.rem(yy, 2) + start, size), :]

    def xsem(yy, xx, u):
        return x_rs.at[16 * lax.rem(yy, 2) + 4 * xx + u]

    def wslot(zz, yy, r):
        return wbuf.at[2 * (4 * zz + yy) + r, :, pl.ds(0, 640)]

    def wsem(zz, yy, r):
        return w_rs.at[2 * (4 * zz + yy) + r]

    def woslot(zz, yy, cc, half=None):
        block = wo.at[zz, 2 * lax.rem(yy, 2) + cc]
        return block if half is None else block.at[pl.ds(256 * half, 256), :]

    def wosem(zz, yy, cc):
        return wo_rs.at[4 * zz + 2 * lax.rem(yy, 2) + cc]

    def own_x(u):
        start, size = PARTS[u]
        return x_v.at[pl.ds(start, size), :], xslot(y, x, u), xsem(y, x, u)

    def own_x_along_y(u):
        src, dst, sem = own_x(u)
        for i, yy in enumerate((yp, ym)):
            remote(src, dst, x_ss.at[12 + 2 * u + i], sem, dev(z, yy, x, kh), c == u // 2)

    def both(p, q):
        return jnp.logical_and(p, q)

    wo_own = wo.at[z, 2 * yodd + c]
    own_sem = wo_rs.at[4 * z + 2 * yodd + c]

    def own_wo(tos, at):
        for half, ref in enumerate((op_in, od_in)):
            part = wo_own.at[pl.ds(256 * half, 256), :]
            for i, to in enumerate(tos):
                remote(wo_v.at[half], part, wo_ss.at[at + 2 * half + i], own_sem, to)

    yn = 2 * c + 1 - yodd
    yo = 2 * c + yodd
    from_below = mod4(yn + 1) == y
    relay_half = jnp.where(from_below, 0, 1)
    y_next = jnp.where(from_below, yp, ym)
    xf_n, wf_n, wof_n = iter(range(64)), iter(range(64)), iter(range(64))
    x_ring = (dev(z, y, xp, c), dev(z, y, xm, c))
    y_ring = (dev(z, yp, x, c), dev(z, ym, x, c))
    z_ring = (dev(zp, y, x, c), dev(zm, y, x, c))
    y_relay = (relay_half, dev(z, y_next, x, c))
    x_relay = {3: (0, x_ring[0]), 1: (1, x_ring[1])}
    z_relay = {3: (0, z_ring[0]), 1: (1, z_ring[1])}
    x_at, z_at = (x, xp, x2, xm), (z, zp, z2, zm)
    cases = {"n": (yn, None), "h": (yo, home), "a": (yo, away)}
    seen = set()

    def take(key, slot, sem, cond=None):
        if key in seen:
            return
        seen.add(key)
        if cond is None:
            arrived(slot, sem)
        else:
            @pl.when(cond)
            def _():
                arrived(slot, sem)

    def x_take(case, d, u):
        yy, cond = cases[case]
        take(("x", case, d, u), xslot(yy, x_at[d], u), xsem(yy, x_at[d], u), cond)

    def x_pass(case, d, u, tos, relay=None):
        x_take(case, d, u)
        yy, cond = cases[case]
        slot, sem = xslot(yy, x_at[d], u), xsem(yy, x_at[d], u)
        for to in tos:
            remote(slot, slot, xf_ss.at[next(xf_n)], sem, to, cond)
        if relay is not None:
            half, to = relay
            part = xslot(yy, x_at[d], u, half)
            remote(part, part, xf_ss.at[next(xf_n)], sem, to, cond)

    def o_take(case, d, cc):
        yy, cond = cases[case]
        take(("o", case, d, cc), woslot(z_at[d], yy, cc), wosem(z_at[d], yy, cc), cond)

    def o_pass(case, d, cc, tos, relay=None):
        o_take(case, d, cc)
        yy, cond = cases[case]
        slot, sem = woslot(z_at[d], yy, cc), wosem(z_at[d], yy, cc)
        for to in tos:
            remote(slot, slot, wof_ss.at[next(wof_n)], sem, to, cond)
        if relay is not None:
            half, to = relay
            part = woslot(z_at[d], yy, cc, half)
            remote(part, part, wof_ss.at[next(wof_n)], sem, to, cond)

    def w_take(d, e, r, tag):
        yy = mod4(me_y + e)
        take((tag, d, e), wslot(z_at[d], yy, r), wsem(z_at[d], yy, r))

    def w_pass(d, e, tos):
        w_take(d, e, c, "w")
        yy = mod4(me_y + e)
        slot, sem = wslot(z_at[d], yy, c), wsem(z_at[d], yy, c)
        for to in (*tos, partner):
            remote(slot, slot, wf_ss.at[next(wf_n)], sem, to)

    def fill(i, carry):
        rows = pl.ds(pl.multiple_of(512 * i, 512), 512)
        both_cols = dot(rates_v[:, rows], pick, ((0,), (0,))).astype(BF16)
        wbuf[pl.ds(4 * i, 4), :, 640:768] = both_cols.reshape(4, 128, 128)
        return carry

    head = 4 * x + y
    row32, col32 = iota((32, 128), 0), iota((32, 128), 1)
    pick = jnp.logical_or(
        jnp.logical_and(row32 == head, col32 == 0),
        jnp.logical_and(row32 == head + 16, col32 == 1),
    ).astype(BF16)

    def project(i):
        total = acc[...]
        for k in (0, 1):
            gains = [gain_f[pl.ds(8 * i + 4 * k + q, 1), :] for q in range(4)]
            gain = jnp.concatenate(gains, axis=1)
            for b in range(4):
                rows = slice(128 * b, 128 * b + 128)
                v = xbuf[2 * i + k, rows, :].astype(F32)
                sq = v * v
                ssq[rows, :] += (
                    (sq[:, 0:128] + sq[:, 128:256]) + (sq[:, 256:384] + sq[:, 384:512])
                )
                xg[k, rows, :] = (v * gain).astype(BF16)
            total = total + dot(xg[k], wbuf[pl.ds(8 * i + 4 * k, 4)].reshape(512, 768))
        acc[...] = total

    ii, jj = iota((256, 256), 0), iota((256, 256), 1)
    diff = jnp.bitwise_xor(ii, jj)
    lower = ii > jj
    causal = ii >= jj
    upto = (ii <= jj).astype(F32)
    eye = (ii == jj).astype(F32)

    def row_scale(b):
        total = jnp.sum(ssq[256 * b : 256 * b + 256, :], axis=-1, keepdims=True)
        return lax.rsqrt(total * (1.0 / 4096.0) + EPS)

    prev_to = dev(jnp.where(c == 0, z, zp), y, x, 1 - c)
    last = jnp.logical_and(z == 3, c == 1)
    first = jnp.logical_and(z == 0, c == 0)
    prev_dst = ap.at[pl.ds(256, 16), pl.ds(0, 128)]
    heads = []
    maps = []

    def spread_out(src, dst, rsem, ssem):
        cols = pl.ds(128 * y, 128)

        @pl.when(home)
        def _():
            dst[0:256, cols] = src[pl.ds(256 * yodd, 256), :]

        for j in (0, 1):
            to_y = 2 * c + j
            here = to_y == y
            rows = pl.ds(256 * j, 256)
            remote(
                src.at[rows, :], dst.at[pl.ds(0, 256), cols], ssem.at[3 * j],
                rsem.at[y], partner, here,
            )
            for r in (0, 1):
                remote(
                    src.at[pl.ds(256 * j + 128 * r, 128), :],
                    dst.at[pl.ds(128 * r, 128), cols],
                    ssem.at[3 * j + 1 + r], rsem.at[y], dev(z, to_y, x, r),
                    jnp.logical_not(here),
                )

    def t_x():
        for half in (1, 0):
            for cc in (0, 1):
                u = 2 * cc + half
                src, dst, sem = own_x(u)
                for i, xx in enumerate((xp, xm)):
                    remote(src, dst, x_ss.at[3 * u + i], sem, dev(z, y, xx, kh), c == cc)
                mine = c == cc
                remote(src, dst, x_ss.at[3 * u + 2], sem, partner, both(mine, away))

                @pl.when(both(mine, home))
                def _(u=u, dst=dst, sem=sem):
                    start, size = PARTS[u]
                    pltpu.make_async_copy(x_in.at[pl.ds(start, size), :], dst, sem).start()

    def t_y():
        for u in (0, 1, 2):
            own_x_along_y(u)

    def t_s():
        for j in (0, 1):
            same = yodd == j
            for r in (0, 1):
                far = dev(z, yp if r == 0 else ym, x, r)
                for n, ref in enumerate((wp_in, wq_in, wk_in, wv_in, wg_in)):
                    src = w_v.at[n, pl.ds(128 * r, 128), pl.ds(128 * j, 128)]
                    dst = w_stage.at[:, pl.ds(128 * n, 128)]
                    remote(src, dst, w_ss.at[10 * j + 5 * r + n], ws_rs.at[0], far, both(away, same))

    def t_w():
        for j in (0, 1):
            same = yodd == j
            head_y = 2 * c + j
            for r in (0, 1):
                here = both(both(home, same), c == r)
                direct = jnp.logical_not(jnp.logical_or(here, both(away, same)))
                for n, ref in enumerate((wp_in, wq_in, wk_in, wv_in, wg_in)):
                    src = ref.at[pl.ds(128 * r, 128), pl.ds(128 * j, 128)]
                    dst = wbuf.at[2 * sp + r, :, pl.ds(128 * n, 128)]
                    here_v = w_v.at[n, pl.ds(128 * r, 128), pl.ds(128 * j, 128)]
                    remote(
                        here_v, dst, w_ss.at[20 + 10 * j + 5 * r + n], wsem(z, y, r),
                        dev(z, head_y, x, r), direct,
                    )

                    @pl.when(here)
                    def _(src=src, dst=dst, r=r):
                        pltpu.make_async_copy(src, dst, wsem(z, y, r)).start()

        for half, ref in enumerate((op_in, od_in)):
            part = wo_own.at[pl.ds(256 * half, 256), :]
            remote(wo_v.at[half], part, wo_ss.at[8 + half], own_sem, partner, away)

            @pl.when(home)
            def _(ref=ref, part=part):
                pltpu.make_async_copy(ref, part, own_sem).start()

    def t_b():
        for i, (src, dst) in enumerate(loads):
            pltpu.make_async_copy(src, dst, in_rs.at[i]).wait()
        pk_src[0:2, :] = factor_v[...]
        pk_src[2:4, :] = offset_v[...]
        for j in (0, 1):
            for at, ref in ((4, hld_v), (6, dlb_v), (8, wlb_v)):
                pk_src[at + j : at + j + 1, :] = jnp.broadcast_to(ref[0:1, j : j + 1], (1, 256))
        pk_src[10:11, :] = pscale_v[...]
        for j in (0, 1):
            head_y = 2 * c + j
            self_here = jnp.logical_and(head_y == y, home)
            remote(
                pk_src, packb.at[yodd], pk_ss.at[j], pk_rs.at[yodd], dev(z, head_y, x, kh),
                jnp.logical_not(self_here),
            )

            @pl.when(self_here)
            def _():
                packb[yodd] = pk_src[...]

        remote(pm_in.at[yodd], pmb, pm_ss.at[0], pm_rs.at[0], partner, home)

        @pl.when(home)
        def _():
            pltpu.make_async_copy(pm_in.at[yodd], pmb, pm_rs.at[0]).start()

    def stage():
        arrived(w_stage, ws_rs.at[0])
        stage_from = jnp.where(c == 0, ym, yp)
        stage_to = jnp.where(c == 0, yp, ym)
        stage_dst = wbuf.at[2 * (4 * z + stage_from) + c, :, pl.ds(0, 640)]
        remote(w_stage, stage_dst, w_ss.at[40], wsem(z, stage_from, c), dev(z, stage_to, x, c))

    def start_rates():
        lax.fori_loop(0, 8, fill, 0)
        gain_f[...] = gain_v[...].astype(F32)
        ssq[...] = jnp.zeros_like(ssq)
        acc[...] = jnp.zeros_like(acc)

    gap = mod4(x - z)

    def depth(parts, ds):
        for d in ds:
            for case in "nha":
                for u in range(4):
                    x_take(case, d, u)
            for e in (0, 1, 2, 3):
                w_take(d, e, c, "w")
                w_take(d, e, 1 - c, "p")
        for i in parts:
            project(i)

    def early():
        first_part = jnp.where(gap == 2, xp, x)
        depth((first_part, jnp.where(gap == 2, xm, jnp.where(gap == 0, xp, z))), (0, 1, 3))

    def late_x():
        for case in "nha":
            for u in range(4):
                x_take(case, 2, u)
        project(jnp.where(gap == 0, xm, jnp.where(gap == 2, z, x2)))

    def late():
        depth((jnp.where(gap == 0, x2, jnp.where(gap == 2, x, z2)),), (2,))

    def delta_heads():
        pl.semaphore_wait(near, 4)
        for b in (0, 1):
            @pl.when(jnp.logical_or(away, yodd != b))
            def _(b=b):
                arrived(packb.at[b], pk_rs.at[b])
        arrived(pmb, pm_rs.at[0])

        scale = [row_scale(0), row_scale(1)]

        for b in (0, 1):
            pad[16 + 256 * b : 272 + 256 * b, :] = acc[256 * b : 256 * b + 256, 0:128] * scale[b]
        prev_src[...] = pad[512:528, :].astype(BF16)
        remote(prev_src, prev_dst, prev_ss.at[0], prev_rs.at[0], prev_to, jnp.logical_not(last))

        for b in (0, 1):
            rows = slice(256 * b, 256 * b + 256)
            s = scale[b]
            q = unit(silu(acc[rows, 128:256] * s)) * HD ** (-0.5)
            k = unit(silu(acc[rows, 256:384] * s))
            v = silu(acc[rows, 384:512] * s)
            rate = acc[rows, 640:768] * s
            table = packb[b]
            of = lambda r: jnp.where(yodd == 0, table[r : r + 1, :], table[r + 1 : r + 2, :])
            factor, offset, hld, dlb, wlb = (of(r) for r in (0, 2, 4, 6, 8))
            pre = rate.T[0:1, :] + dlb
            soft = jnp.maximum(pre, 0.0) + jnp.log1p(jnp.exp(-jnp.abs(pre)))
            log_decay = -jnp.exp(hld) * soft * factor + offset
            run_row = dot(jnp.broadcast_to(log_decay, (8, 256)), upto, precision=HIGHEST)[0:1, :]
            run = jnp.broadcast_to(run_row, (128, 256)).T
            beta = jax.nn.sigmoid(rate[:, 1:2] + wlb[:, 0:1])
            spread = jnp.concatenate([run, run], axis=1) - run_row
            decay = jnp.where(causal, jnp.exp(jnp.where(causal, spread, 0.0)), 0.0)
            k16, q16 = k.astype(BF16), q.astype(BF16)
            low = jnp.where(lower, dot(k16, k16, ((1,), (1,))) * (decay * beta), 0.0)
            scores = (dot(q16, k16, ((1,), (1,))) * decay).astype(BF16)
            inverse = eye - jnp.where(diff == 1, low, 0.0)
            grown = jnp.exp(run)
            kb = k * beta
            low_s[b] = low
            inv_s[b] = inverse
            heads.append(dict(q=q, k=k, v=v, scores=scores, run=run, grown=grown, kb=kb, beta=beta))

    def level_step(level):
        mask = jnp.right_shift(diff, level) == 1
        mids = []
        for b in (0, 1):
            off = jnp.where(mask, low_s[b], 0.0).astype(BF16)
            mids.append(dot(off, inv_s[b].astype(BF16)).astype(BF16))
        for b, mid in enumerate(mids):
            inv_s[b] = inv_s[b] - dot(inv_s[b].astype(BF16), mid)

    def delta_maps():
        for b, h in enumerate(heads):
            rows = slice(256 * b, 256 * b + 256)
            rhs = jnp.concatenate([h["v"] * h["beta"], h["kb"] * h["grown"]], axis=1)
            uw = rhs + dot((inv_s[b] - eye).astype(BF16), rhs.astype(BF16))
            uw16 = uw.astype(BF16)
            both = dot(h["scores"], uw16)
            o0[rows, :] = both[:, 0:128]
            pmx[rows, :] = (h["q"] * h["grown"] - both[:, 128:256]).astype(BF16)
            last_run = h["run"][255:256, :]
            kd = (h["k"] * jnp.exp(last_run - h["run"])).astype(BF16)
            ku = dot(kd, uw16, ((0,), (0,)))
            keep = jnp.exp(last_run)
            maps.append((keep, ku[:, 128:256].astype(BF16), ku[:, 0:128]))

        eye128 = (iota((128, 128), 0) == iota((128, 128), 1)).astype(F32)
        keep0, kw0, b0 = maps[0]
        keep1, kw1, b1 = maps[1]
        m0 = eye128 * keep0 - kw0.astype(F32)
        kw0_s[...] = kw0
        b0_s[...] = b0
        keep_s[0:1, :] = keep0
        first_map = jnp.concatenate([m0, b0], axis=1)
        keep1w = jnp.concatenate([keep1, keep1], axis=1)
        core_map = keep1w * first_map - dot(kw1, first_map.astype(BF16))
        core_map = core_map + jnp.concatenate([jnp.zeros_like(b1), b1], axis=1)
        stc[c] = core_map.astype(BF16)
        remote(stc.at[c], stc.at[c], st_ss.at[0], st_rs.at[c], partner)

    def join_maps():
        arrived(stc.at[1 - c], st_rs.at[1 - c])
        one = stc[1]
        chip_map = dot(one[:, 0:128], stc[0])
        chip_map = chip_map + jnp.concatenate([jnp.zeros((128, 128), F32), one[:, 128:256].astype(F32)], axis=1)
        stz_src[...] = chip_map.astype(BF16)
        for d in (2, 1, 3):
            remote(
                stz_src, stz.at[z], stz_ss.at[d - 1], stz_rs.at[z],
                dev(mod4(z + d), y, x, c), z + d <= 3,
            )

    def pool_part():
        @pl.when(first)
        def _():
            pad[0:16, :] = jnp.zeros((16, 128), F32)

        @pl.when(jnp.logical_not(first))
        def _():
            arrived(prev_dst, prev_rs.at[0])
            pad[0:16, :] = ap[256:272, 0:128].astype(F32)

        window = jnp.left_shift(2, y)
        base = 512 * (2 * z + c)
        for b in (0, 1):
            at = 256 * b
            sums = pad[16 + at : 272 + at, :]
            here = sums
            for lag in range(1, 16):
                part = pad[16 + at - lag : 272 + at - lag, :]
                sums = sums + part * jnp.where(lag < window, 1.0, 0.0)
            counts = jnp.minimum(base + at + iota((256, 128), 0) + 1, window).astype(F32)
            pooled = (sums / counts - here).astype(BF16)
            row = packb[b]
            pscale = jnp.where(yodd == 0, row[10:11, 0:128], row[10:11, 128:256])
            pool_src[at : at + 256, :] = (dot(pooled, pmb[...]) * pscale).astype(BF16)

        spread_out(pool_src, ap, ap_rs, ap_ss)

    def state_in():
        state_s[...] = jnp.zeros((128, 128), F32)

        def absorb(part):
            moved = dot(part[:, 0:128], state_s[...].astype(BF16))
            state_s[...] = moved + part[:, 128:256].astype(F32)

        for i in (0, 1, 2):
            @pl.when(i < z)
            def _(i=i):
                arrived(stz.at[i], stz_rs.at[i])
                absorb(stz[i])

        @pl.when(c == 1)
        def _():
            absorb(stc[0])

    def finish():
        hng = hng_v[...]
        for b in (0, 1):
            rows = slice(256 * b, 256 * b + 256)
            s16 = state_s[...].astype(BF16)
            o = o0[rows, :] + dot(pmx[rows, :], s16)
            gate = silu(acc[rows, 512:640] * row_scale(b))
            norm = lax.rsqrt(jnp.mean(o * o, axis=-1, keepdims=True) + EPS)
            delta_src[rows, :] = (o * norm * hng * gate).astype(BF16)
            if b == 0:
                state_s[...] = keep_s[0:1, :] * state_s[...] - dot(kw0_s[...], s16) + b0_s[...]

        spread_out(delta_src, ad, ad_rs, ad_ss)

    def pass_on(dst, rsem, fsem):
        for i, d in enumerate((1, 3, 2)):
            yy = mod4(me_y + d)
            part = dst.at[pl.ds(128 * c, 128), pl.ds(128 * yy, 128)]
            arrived(part, rsem.at[yy])
            remote(part, part, fsem.at[i], rsem.at[4 + yy], partner)

    def from_partner(dst, rsem):
        for d in (1, 3, 2):
            yy = mod4(me_y + d)
            part = dst.at[pl.ds(128 * (1 - c), 128), pl.ds(128 * yy, 128)]
            arrived(part, rsem.at[4 + yy])

        @pl.when(away)
        def _():
            arrived(dst.at[pl.ds(0, 256), pl.ds(128 * me_y, 128)], rsem.at[me_y])

    def rest_of_output_weights():
        for d in range(4):
            for case in "nha":
                for cc in (0, 1):
                    o_take(case, d, cc)
        from_partner(ap, ap_rs)
        from_partner(ad, ad_rs)

    ops = dict(
        TX=t_x, GP=lambda: pass_on(ap, ap_rs, apf_ss),
        GD=lambda: pass_on(ad, ad_rs, adf_ss), TY=t_y, TS=t_s, TW=t_w, TB=t_b, ST=stage, FILL=start_rates, EARLY=early,
        LATEX=late_x, LATE=late, heads=delta_heads, level=level_step, maps=delta_maps, join=join_maps,
        pool=pool_part, state=state_in, finish=finish, WOALL=rest_of_output_weights,
        W0=lambda e: w_pass(0, e, z_ring),
        WL=lambda d, e: w_pass(d, e, (z_relay[d][1],) if (d == 3) == (e in (0, 2)) else ()),
        WT=lambda e: w_pass(2, e, ()),
        XA=lambda u: x_pass("n", 0, u, x_ring, y_relay),
        XO=lambda u: x_pass("a", 0, u, x_ring),
        XB=lambda d: x_pass("h", d, 3, y_ring, x_relay[d]),
        XB2=lambda: x_pass("h", 2, 3, y_ring),
        XN=lambda d: x_pass("n", d, 3, (), y_relay),
        XR=lambda case, d, u: x_pass(case, d, u, (), x_relay[d]),
        OXY=lambda: own_x_along_y(3),
        OY=lambda: own_wo((dev(z, yp, x, kh), dev(z, ym, x, kh)), 4),
        OZ=lambda: own_wo((dev(zp, y, x, kh), dev(zm, y, x, kh)), 0),
        OA=lambda: o_pass("n", 0, 1, z_ring, y_relay),
        OO=lambda: o_pass("a", 0, 1, z_ring),
        OB=lambda d: o_pass("h", d, 0, y_ring, z_relay[d]),
        OB2=lambda: o_pass("h", 2, 0, y_ring),
        ON=lambda d: o_pass("n", d, 0, (), y_relay),
        OR=lambda case, d: o_pass(case, d, 1, (), z_relay[d]),
    )
    for name, *args in SCHEDULE:
        ops[name](*args)

    def piece(zz):
        halves = []
        for j in (0, 1):
            part = None
            for cc in (0, 1):
                cols = slice(256 * cc, 256 * cc + 256)
                term = dot(ap[0:256, cols], wo[zz, 2 * j + cc, 0:256, :])
                term = term + dot(ad[0:256, cols], wo[zz, 2 * j + cc, 256:512, :])
                part = term if part is None else part + term
            halves.append(part)
        return jnp.concatenate(halves, axis=1)

    top, bottom = pl.ds(0, 128), pl.ds(128, 128)
    to_p, to_m = dev(z, y, xp, c), dev(z, y, xm, c)
    rs2[...] = piece(x2).astype(BF16)
    remote(rs2.at[top, :], rl.at[0], rs_ss.at[0], rs_rs.at[0], to_p)
    remote(rs2.at[bottom, :], rl.at[1], rs_ss.at[1], rs_rs.at[1], to_m)
    up_s[...] = piece(xp)
    rsp[128:256, :] = up_s[128:256, :].astype(BF16)
    remote(rsp.at[bottom, :], rin.at[0, bottom, :], rs_ss.at[2], rs_rs.at[2], to_p)
    down_s[...] = piece(xm)
    rsm[0:128, :] = down_s[0:128, :].astype(BF16)
    remote(rsm.at[top, :], rin.at[1, top, :], rs_ss.at[3], rs_rs.at[3], to_m)
    arrived(rl.at[0], rs_rs.at[0])
    rsp[0:128, :] = (up_s[0:128, :] + rl[0].astype(F32)).astype(BF16)
    remote(rsp.at[top, :], rin.at[0, top, :], rs_ss.at[4], rs_rs.at[4], to_p)
    arrived(rl.at[1], rs_rs.at[1])
    rsm[128:256, :] = (down_s[128:256, :] + rl[1].astype(F32)).astype(BF16)
    remote(rsm.at[bottom, :], rin.at[1, bottom, :], rs_ss.at[5], rs_rs.at[5], to_m)
    mine = piece(x)
    arrived(rin.at[0, bottom, :], rs_rs.at[2])
    arrived(rin.at[1, top, :], rs_rs.at[3])
    arrived(rin.at[0, top, :], rs_rs.at[4])
    arrived(rin.at[1, bottom, :], rs_rs.at[5])
    out_ref[...] = (mine + rin[0].astype(F32) + rin[1].astype(F32)).astype(BF16)

    for end in ends:
        end()


def per_device(
    inputs, input_norm_gain, pooling_input_weight, query_weight, key_weight,
    value_weight, gate_weight, decay_weight, strength_weight, pooling_group_map,
    pooling_scale, head_log_decay, decay_logit_bias, write_logit_bias,
    decay_position_factor, decay_position_offset, head_norm_gain,
    pooling_output_weight, delta_output_weight,
):
    dma = pltpu.SemaphoreType.DMA
    vmem = pltpu.VMEM
    hbm = pl.BlockSpec(memory_space=pl.ANY)
    local = pl.BlockSpec(memory_space=pltpu.VMEM)
    return pl.pallas_call(
        kernel,
        out_shape=pltpu.VMEM((256, 512), BF16),
        in_specs=[hbm] * 19,
        out_specs=local,
        scratch_shapes=[
            vmem((1, 2), F32),
            vmem((1, 2), F32),
            vmem((1, 2), F32),
            vmem((32, 128), BF16),
            vmem((2, 256), F32),
            vmem((2, 256), F32),
            vmem((1, 256), F32),
            vmem((1, 128), F32),
            vmem((32, 4096), BF16),
            vmem((256, 512), BF16),
            vmem((5, 256, 256), BF16),
            vmem((2, 256, 256), BF16),
            vmem((8, 512, 512), BF16),
            vmem((32, 128, 768), BF16),
            vmem((4, 4, 512, 256), BF16),
            vmem((32, 128), F32),
            vmem((16, 256), F32),
            vmem((2, 16, 256), F32),
            vmem((128, 128), BF16),
            vmem((2, 512, 512), BF16),
            vmem((512, 768), F32),
            vmem((512, 128), F32),
            vmem((128, 640), BF16),
            vmem((2, 128, 256), BF16),
            vmem((128, 256), BF16),
            vmem((4, 128, 256), BF16),
            vmem((528, 128), F32),
            vmem((512, 128), BF16),
            vmem((512, 128), BF16),
            vmem((16, 128), BF16),
            vmem((272, 512), BF16),
            vmem((256, 512), BF16),
            vmem((256, 512), BF16),
            vmem((256, 512), BF16),
            vmem((256, 512), BF16),
            vmem((2, 128, 512), BF16),
            vmem((2, 256, 512), BF16),
            vmem((512, 128), F32),
            vmem((512, 128), BF16),
            vmem((128, 128), BF16),
            vmem((128, 128), F32),
            vmem((8, 128), F32),
            vmem((2, 256, 256), F32),
            vmem((2, 256, 256), F32),
            vmem((256, 512), F32),
            vmem((256, 512), F32),
            vmem((128, 128), F32),
            dma((10,)), dma((8,)), pltpu.SemaphoreType.REGULAR, dma((1,)), dma((32,)), dma((32,)), dma((16,)), dma((2,)), dma((1,)), dma((2,)),
            dma((4,)), dma((1,)), dma((8,)), dma((8,)), dma((6,)),
            dma((20,)), dma((48,)), dma((41,)), dma((32,)), dma((10,)), dma((32,)),
            dma((2,)), dma((1,)), dma((1,)), dma((3,)), dma((1,)),
            dma((6,)), dma((6,)), dma((3,)), dma((3,)), dma((6,)),
        ],
        compiler_params=pltpu.CompilerParams(
            collective_id=0, has_side_effects=True, vmem_limit_bytes=60 * 1024 * 1024
        ),
    )(
        inputs, pooling_input_weight, query_weight, key_weight, value_weight,
        gate_weight, pooling_output_weight, delta_output_weight, pooling_group_map,
        head_log_decay[None], decay_logit_bias[None], write_logit_bias[None],
        input_norm_gain.reshape(32, 128), decay_position_factor.T, decay_position_offset.T,
        pooling_scale[None], head_norm_gain[None], decay_weight.T, strength_weight.T,
    )


def solution(mesh):
    rows, heads = P("sp", "tp"), P("tp")
    in_specs = (
        rows, P(), rows, rows, rows, rows, rows, P(), P(), P("tp", None, None),
        heads, heads, heads, heads, rows, rows, P(), P("tp", "sp"), P("tp", "sp"),
    )
    return jax.shard_map(
        per_device, mesh=mesh, in_specs=in_specs, out_specs=rows, check_vma=False
    )
```
